512 devices in a mesh: sp: 256 (over z, y, x), tp: 2 (over core).
Axes of the slice: x: 4, y: 4, z: 16, core: 2. Of those that a mesh axis runs over, the one named last changes fastest.
Arguments:
- stream: bfloat16 [1024, 131072], P('tp', 'sp'), may hold values from -6 to 6
- norm_gain: float32 [2, 1024], replicated, may hold values from 0.1 to 1.9
- w_value: bfloat16 [2, 512, 1024], P(None, 'tp'), may hold values from -0.1875 to 0.1875
- w_gate: bfloat16 [2, 512, 1024], P(None, 'tp'), may hold values from -0.1875 to 0.1875
- conv_taps: bfloat16 [2, 512, 255], P(None, 'tp'), may hold values from -0.375 to 0.375
- group_gain: float32 [2, 512], P(None, 'tp'), may hold values from 0.1 to 1.9
- group_shift: float32 [2, 512], P(None, 'tp'), may hold values from -3 to 3
- w_out: bfloat16 [2, 1024, 512], P(None, 'tp'), may hold values from -0.25 to 0.25
Outputs:
- result: bfloat16 [1024, 131072], P('tp', 'sp')
The draws below stay inside these ranges and needn't reach their ends.
All inputs are finite; a program needn't handle non-finite values.
Results may differ from the reference program's by a relative error of at most 0.014.
Values may be sent and summed in bfloat16 or wider, within the bound.
A program may use at most 64 MiB of HBM per device.

```python
import math
import jax
import jax.numpy as jnp
from jax import lax

D = 1024
C = 512
GROUP_DIM = 128
KERNEL = 255
LAYERS = 2
TOK_DEV = 512
TOKENS = 131072
N_SP = 256


def shard_levels(stream_key, dims, split, least, top_value):
    def one(position, blocks):
        heights = jax.random.uniform(jax.random.fold_in(jax.random.fold_in(stream_key, 6), position), (blocks,), jnp.float32, least / len(split), top_value / len(split))
        return jnp.repeat(jnp.exp(heights), dims[position] // blocks).reshape((-1,) + (1,) * (len(dims) - position - 1))

    factor_of = one(*split[0])
    for cut in split[1:]:
        factor_of = factor_of * one(*cut)
    return factor_of


def noise(rng, extent, width, most, pieces=(), kind=jnp.bfloat16):
    level = shard_levels(rng, extent, pieces, -0.22, 0.18) if pieces else 1.0
    drawn = jax.random.normal(rng, extent, jnp.float32) * width * level
    return jnp.minimum(jnp.maximum(drawn, -most), most).astype(kind)


def setup_inputs(seed: int = 0) -> dict:
    key_list = jax.random.split(jax.random.key(seed), 9)
    return {
        "stream": noise(key_list[0], (D, TOKENS), 1.0, 6.0, ((0, 2), (1, 256))),
        "norm_gain": jnp.clip(1.0 + 0.18 * jax.random.normal(key_list[1], (LAYERS, D), jnp.float32), 0.1, 1.9),
        "w_value": noise(key_list[2], (LAYERS, C, D), D ** -0.5, 0.1875, ((1, 2),)),
        "w_gate": noise(key_list[3], (LAYERS, C, D), D ** -0.5, 0.1875, ((1, 2),)),
        "conv_taps": noise(key_list[4], (LAYERS, C, KERNEL), KERNEL ** -0.5, 0.375, ((1, 2),)),
        "group_gain": jnp.clip(1.0 + 0.18 * jax.random.normal(key_list[5], (LAYERS, C), jnp.float32), 0.1, 1.9),
        "group_shift": noise(key_list[6], (LAYERS, C), 0.5, 3.0, ((1, 2),), jnp.float32),
        "w_out": noise(key_list[7], (LAYERS, D, C), C ** -0.5, 0.25, ((1, 2),)),
    }


RMS_EPS = 1e-06
LN_EPS = 1e-05

def one_layer(stream, gain, wv, wg, taps, ggain, gshift, wo):
    rim_width = (KERNEL - 1) // 2
    total = stream.shape[1]
    block = TOK_DEV * math.gcd(N_SP, 8)
    nblocks = total // block

    def gated_block(index):
        start = (index * block).astype(jnp.int32)
        piece = lax.dynamic_slice_in_dim(stream, start, block, 1)
        widened = piece.astype(jnp.float32)
        inverse_rms = lax.rsqrt(lax.optimization_barrier(jnp.mean(widened * widened, axis=0, keepdims=True)) + RMS_EPS)
        normed = (widened * inverse_rms * gain[:, None]).astype(jnp.bfloat16)
        projected = jnp.dot(wv, normed, preferred_element_type=jnp.float32).astype(jnp.bfloat16)
        gate_proj = jnp.dot(wg, normed, preferred_element_type=jnp.float32).astype(jnp.bfloat16)
        return (projected.astype(jnp.float32) * jax.nn.sigmoid(gate_proj.astype(jnp.float32))).astype(jnp.bfloat16)
    stacked = lax.map(gated_block, jnp.arange(nblocks, dtype=jnp.int32))
    gated = jnp.moveaxis(stacked, 0, 1).reshape(C, total)
    padded = jnp.pad(gated, ((0, 0), (rim_width, rim_width)))
    taps_wide = taps.astype(jnp.float32)

    def out_block(index):
        start = (index * block).astype(jnp.int32)
        window = lax.dynamic_slice_in_dim(padded, start, block + 2 * rim_width, 1)

        def add_tap(tap, running):
            shifted = lax.dynamic_slice_in_dim(window, tap.astype(jnp.int32), block, 1)
            column = lax.dynamic_slice_in_dim(taps_wide, tap.astype(jnp.int32), 1, 1)
            return running + column * shifted.astype(jnp.float32)
        filtered = lax.fori_loop(0, KERNEL, add_tap, jnp.zeros((C, block), jnp.float32))
        grouped = filtered.reshape(C // GROUP_DIM, GROUP_DIM, block)
        group_mean = lax.optimization_barrier(jnp.mean(grouped, axis=1, keepdims=True))
        centred = grouped - group_mean
        scaled = centred * lax.rsqrt(lax.optimization_barrier(jnp.mean(centred * centred, axis=1, keepdims=True)) + LN_EPS)
        scaled = scaled.reshape(C, block) * ggain[:, None] + gshift[:, None]
        activated = jax.nn.silu(scaled).astype(jnp.bfloat16)
        branch = jnp.dot(wo, activated, preferred_element_type=jnp.float32)
        piece = lax.dynamic_slice_in_dim(stream, start, block, 1)
        return (piece.astype(jnp.float32) + branch).astype(jnp.bfloat16)
    outs = lax.map(out_block, jnp.arange(nblocks, dtype=jnp.int32))
    return jnp.moveaxis(outs, 0, 1).reshape(stream.shape[0], total)

def reference(stream, norm_gain, w_value, w_gate, conv_taps, group_gain, group_shift, w_out):
    for layer_index in range(LAYERS):
        stream = one_layer(stream, norm_gain[layer_index], w_value[layer_index], w_gate[layer_index], conv_taps[layer_index], group_gain[layer_index], group_shift[layer_index], w_out[layer_index])
    return stream
```

```python
import jax
import jax.numpy as jnp
import numpy as np
from jax import lax
from jax.sharding import PartitionSpec as P

GROUP_DIM = 128


RMS_EPS = 1e-06
LN_EPS = 1e-05


def in_order(parts, dim):
    parts = jnp.moveaxis(parts, 0, dim)
    shape = parts.shape
    return parts.reshape(*shape[:dim], shape[dim] * shape[dim + 1], *shape[dim + 2 :])


def sent_to_all(value, axis):
    count = lax.axis_size(axis)
    return lax.all_to_all(
        jnp.broadcast_to(value[None], (count, *value.shape)), axis, 0, 0, tiled=True
    )


def gathered_copies(value, axis, dim):
    return in_order(sent_to_all(value, axis), dim)


def with_halo(cells, sides, width):
    for axis, dim in sides:
        count = lax.axis_size(axis)
        ends = count - 1
        head = lax.slice_in_dim(cells, 0, width, axis=dim)
        tail = lax.slice_in_dim(cells, cells.shape[dim] - width, cells.shape[dim], axis=dim)
        cells = jnp.concatenate(
            [
                lax.ppermute(tail, axis, [(i, (i + 1) % count) for i in range(ends)]),
                cells,
                lax.ppermute(head, axis, [((i + 1) % count, i) for i in range(ends)]),
            ],
            axis=dim,
        )
    return cells


def make_gated(whole, gain, value_weight, gate_weight):
    widened = whole.astype(jnp.float32)
    inverse_rms = lax.rsqrt(jnp.mean(widened * widened, axis=0, keepdims=True) + RMS_EPS)
    normed = (widened * inverse_rms * gain[:, None]).astype(jnp.bfloat16)
    projected = jnp.dot(value_weight, normed, preferred_element_type=jnp.float32).astype(
        jnp.bfloat16
    )
    gate_proj = jnp.dot(gate_weight, normed, preferred_element_type=jnp.float32).astype(
        jnp.bfloat16
    )
    return (projected.astype(jnp.float32) * jax.nn.sigmoid(gate_proj.astype(jnp.float32))).astype(
        jnp.bfloat16
    )


def trig_tables(size, rows, outputs):
    freqs = (np.arange(size // 2) + 0.5) * (2 * np.pi / size)
    angle = np.arange(rows)[:, None] * freqs[None]
    forward = np.concatenate([np.cos(angle), np.sin(angle)], axis=1)
    back = forward[:outputs].T
    return jnp.asarray(forward, jnp.bfloat16), jnp.asarray(back, jnp.bfloat16)


def filter_norm(padded, taps, ggain, gshift):
    channels = taps.shape[0]
    window = padded.shape[1]
    size = -(-window // 256) * 256
    forward, inverse = trig_tables(size, size, window - taps.shape[1] + 1)
    half = size // 2
    spectrum = jnp.dot(padded, forward[:window], preferred_element_type=jnp.float32)
    response = jnp.dot(taps, forward[: taps.shape[1]], preferred_element_type=jnp.float32) * (2.0 / size)
    gr, gs = spectrum[:, :half], spectrum[:, half:]
    hr, hs = response[:, :half], response[:, half:]
    product = jnp.concatenate([gr * hr + gs * hs, gs * hr - gr * hs], axis=1).astype(jnp.bfloat16)
    filtered = jnp.dot(product, inverse, preferred_element_type=jnp.float32)
    tokens_here = filtered.shape[1]
    grouped = filtered.reshape(channels // GROUP_DIM, GROUP_DIM, tokens_here)
    group_mean = jnp.mean(grouped, axis=1, keepdims=True)
    centred = grouped - group_mean
    scaled = centred * lax.rsqrt(jnp.mean(centred * centred, axis=1, keepdims=True) + LN_EPS)
    scaled = scaled.reshape(channels, tokens_here) * ggain[:, None] + gshift[:, None]
    return jax.nn.silu(scaled).astype(jnp.bfloat16)


def body(stream, norm_gain, w_value, w_gate, conv_taps, group_gain, group_shift, w_out):
    rim_width = (conv_taps.shape[2] - 1) // 2
    layers = w_value.shape[0]
    for layer_index in range(layers):
        whole = gathered_copies(stream, "tp", 0)
        gated = make_gated(whole, norm_gain[layer_index], w_value[layer_index], w_gate[layer_index])
        padded = with_halo(gated, (("sp", 1),), rim_width)
        activated = filter_norm(
            padded, conv_taps[layer_index], group_gain[layer_index], group_shift[layer_index]
        )
        out_weight = w_out[layer_index]
        initial = jnp.zeros((out_weight.shape[0], activated.shape[1]), jnp.float32)
        branch = initial + jnp.dot(
            out_weight, gathered_copies(activated, "tp", 0), preferred_element_type=jnp.float32
        )
        stream = (stream.astype(jnp.float32) + branch).astype(jnp.bfloat16)
    return stream


def solution(mesh):
    placed = (
        P("tp", "sp"),
        P(),
        P(None, "tp", None),
        P(None, "tp", None),
        P(None, "tp", None),
        P(None, "tp"),
        P(None, "tp"),
        P(None, "tp", None),
    )
    return jax.shard_map(body, mesh=mesh, in_specs=placed, out_specs=P("tp", "sp"), check_vma=False)
```

```python
import functools

import jax
import jax.numpy as jnp
import numpy as np
from jax import lax
from jax.experimental import pallas as pl
from jax.experimental.pallas import tpu as pltpu
from jax.sharding import PartitionSpec as P

MESH = pl.DeviceIdType.MESH
BLK = 128
SIZE = 512
HALF = SIZE // 2
RMS_EPS = 1e-06
LN_EPS = 1e-05
F32 = jnp.float32
BF16 = jnp.bfloat16


def tables(taps):
    angle = lambda t: np.asarray(t)[:, None] * ((np.arange(HALF) + 0.5) * (2 * np.pi / SIZE))[None]
    trig = lambda t: np.concatenate([np.cos(angle(t)), np.sin(angle(t))], axis=1)
    blocks = [np.arange(BLK) + BLK * b for b in range(4)]
    reach = (taps - 1) // 2
    forward = [np.concatenate([trig(blocks[b]) for b in order]) for order in ((0, 1, 2, 3), (3, 2, 1, 0))]
    back = [
        np.concatenate([trig(blocks[b] - reach).T for b in order], axis=1) * (2.0 / SIZE)
        for order in ((1, 2), (2, 1))
    ]
    return (
        jnp.asarray(np.stack(forward), BF16),
        jnp.asarray(np.stack(back), BF16),
        jnp.asarray(trig(np.arange(taps)), BF16),
    )


def kernel(
    n_sp,
    x_hbm, ng_hbm, wv_hbm, wg_hbm, taps_hbm, gg_hbm, gs_hbm, wo_hbm, fwd_hbm, back_hbm, ftap_hbm,
    o_ref,
    xin, xs, nrm, wvg, wo, taps, ngv, ggv, gsv, ngb, ggb, gsb, resp, fwd, back, ftap,
    g1, g2, gfar, gpar1, gpar2, act, obuf,
    lsem, ssem, rsem,
):
    sp, c = lax.axis_index("sp"), lax.axis_index("tp")
    p = 1 - c
    outer = sp + 2 * c - 1
    has_left = sp > 0
    has_right = sp < n_sp - 1
    has_outer = jnp.logical_and(outer >= 0, outer < n_sp)
    left_count = jnp.where(has_left, 1, 0)
    right_count = jnp.where(has_right, 1, 0)
    layers = wv_hbm.shape[0]

    barrier = pltpu.get_barrier_semaphore()
    pl.semaphore_signal(barrier, inc=1, device_id=(sp, p), device_id_type=MESH)

    @pl.when(has_outer)
    def _():
        for core in range(2):
            pl.semaphore_signal(barrier, inc=1, device_id=(outer, core), device_id_type=MESH)

    local, count = {}, [0]

    def load(name, src, dst):
        copy = pltpu.make_async_copy(src, dst, lsem.at[count[0]])
        count[0] += 1
        copy.start()
        local.setdefault(name, []).append(copy)

    def loaded(name):
        for copy in local[name]:
            copy.wait()

    for b in range(4):
        load("x", x_hbm.at[:, pl.ds(b * BLK, BLK)], xin.at[b])
    load("ng", ng_hbm, ngv)
    load("gg", gg_hbm, ggv.at[c])
    load("gs", gs_hbm, gsv.at[c])
    load("taps", taps_hbm, taps.at[c])
    load("ftap", ftap_hbm, ftap)

    def load_wvg(l):
        for k in range(2):
            load(f"wvg{l}", wv_hbm.at[l, pl.ds(k * BLK, BLK)], wvg.at[l, c, k, 0])
            load(f"wvg{l}", wg_hbm.at[l, pl.ds(k * BLK, BLK)], wvg.at[l, c, k, 1])

    load_wvg(0)
    load("tables", fwd_hbm.at[c], fwd)
    load("tables", back_hbm.at[c], back)
    load("wo0", wo_hbm.at[0], wo.at[0, c])
    load_wvg(1)
    load("wo1", wo_hbm.at[1], wo.at[1, c])

    sent = []

    def remote(k, src, dst, device):
        return pltpu.make_async_remote_copy(
            src_ref=src, dst_ref=dst, send_sem=ssem.at[k], recv_sem=rsem.at[k],
            device_id=device, device_id_type=MESH,
        )

    def to_partner(k, src, dst):
        copy = remote(k, src, dst, (sp, p))
        copy.start()
        sent.append(copy)

    def from_partner(k, dst):
        remote(k, dst, dst, (sp, p)).wait_recv()

    def column(row):
        return jnp.broadcast_to(row, (BLK, BLK)).T

    def spread_groups(h):
        for l in range(layers):
            for b in range(2):
                lanes = slice(b * BLK, (b + 1) * BLK)
                ggb[l, h, lanes] = column(ggv[h, l : l + 1, lanes])
                gsb[l, h, lanes] = column(gsv[h, l : l + 1, lanes])

    def respond(h):
        for l in range(layers):
            resp[l, h] = jnp.dot(taps[h, l], ftap[...], preferred_element_type=F32)

    loaded("ng")
    for l in range(layers):
        for b in range(ngv.shape[1] // BLK):
            rows = slice(b * BLK, (b + 1) * BLK)
            ngb[l, rows] = column(ngv[l : l + 1, rows])
    loaded("gg")
    loaded("gs")
    loaded("taps")
    loaded("ftap")
    respond(c)
    spread_groups(c)
    loaded("x")

    pl.semaphore_wait(barrier, 1 + left_count + right_count)

    NEAR, FAR, XMID, XINN, WVG, WO, TAPS, GG, GS, PAR1, PAR2, OMID, OINN, SR = 0, 2, 3, 4, 5, 7, 9, 10, 11, 12, 13, 14, 15, 16
    near = (slice(None), pl.ds(0, BLK))

    def near_copy(b, send, device):
        return pltpu.make_async_remote_copy(
            src_ref=xin.at[b], dst_ref=xs.at[(c, *near)], send_sem=ssem.at[send], recv_sem=rsem.at[NEAR + c],
            device_id=device, device_id_type=MESH,
        )

    to_left = near_copy(0, NEAR, (sp - 1, 1))
    to_right = near_copy(3, NEAR + 1, (sp + 1, 0))

    @pl.when(has_left)
    def _():
        to_left.start()

    @pl.when(has_right)
    def _():
        to_right.start()

    mid, inn = pl.ds(BLK, BLK), pl.ds(2 * BLK, BLK)
    to_partner(XINN, xin.at[1 + p], xs.at[c, :, inn])
    to_partner(XMID, xin.at[3 * p], xs.at[c, :, mid])
    loaded("wvg0")
    to_partner(WVG, wvg.at[0, c], wvg.at[0, c])
    to_partner(TAPS, taps.at[c], taps.at[c])
    to_partner(GG, ggv.at[c], ggv.at[c])
    to_partner(GS, gsv.at[c], gsv.at[c])
    loaded("wo0")
    to_partner(WO, wo.at[0, c], wo.at[0, c])

    xs[c, :, BLK : 2 * BLK] = xin[3 * c]
    xs[c, :, 2 * BLK : 3 * BLK] = xin[1 + c]

    def normalize(l, blocks):
        for b in blocks:
            lanes = slice(b * BLK, (b + 1) * BLK)
            rows = xs.shape[1]
            total = jnp.zeros((1, BLK), F32)
            for h in range(2):
                wide = xs[h, :, lanes].astype(F32)
                total = total + jnp.sum(wide * wide, axis=0, keepdims=True)
            inverse = lax.rsqrt(total * (1.0 / (2 * rows)) + RMS_EPS)
            for h in range(2):
                wide = xs[h, :, lanes].astype(F32)
                part = slice(h * rows, (h + 1) * rows)
                nrm[part, lanes] = (wide * inverse * ngb[l, part]).astype(BF16)

    def gate(l, h, lanes, dst, scale=None):
        w = wvg[l, h].reshape(4 * BLK, wvg.shape[-1])
        r = jnp.dot(w, nrm[:, lanes], preferred_element_type=F32)
        for k in range(2):
            value = r[2 * k * BLK : (2 * k + 1) * BLK]
            gating = r[(2 * k + 1) * BLK : (2 * k + 2) * BLK]
            out = value * (0.5 * jnp.tanh(0.5 * gating) + 0.5)
            if scale is not None:
                out = out * scale
            dst[h, k * BLK : (k + 1) * BLK, lanes] = out.astype(BF16)

    def filter_norm(l, window, outputs, lanes):
        n = outputs.stop - outputs.start
        for h in range(2):
            w = window(h)
            g = jnp.dot(w, fwd[: w.shape[1]], preferred_element_type=F32)
            gr, gi = g[:, :HALF], g[:, HALF:]
            hr, hi = resp[l, h, :, :HALF], resp[l, h, :, HALF:]
            y = jnp.concatenate([(gr * hr + gi * hi).astype(BF16), (gi * hr - gr * hi).astype(BF16)], axis=1)
            filtered = jnp.dot(y, back[:, outputs], preferred_element_type=F32)
            for k in range(2):
                rows = slice(k * BLK, (k + 1) * BLK)
                f = filtered[rows]
                centred = f - jnp.sum(f, axis=0, keepdims=True) * (1.0 / BLK)
                variance = jnp.sum(centred * centred, axis=0, keepdims=True) * (1.0 / BLK)
                gain, shift = ggb[l, h, rows], gsb[l, h, rows]
                if n > BLK:
                    gain = jnp.concatenate([gain] * (n // BLK), axis=1)
                    shift = jnp.concatenate([shift] * (n // BLK), axis=1)
                s = centred * lax.rsqrt(variance + LN_EPS) * gain + shift
                act[h * 2 * BLK + k * BLK : h * 2 * BLK + (k + 1) * BLK, lanes] = (
                    0.5 * s * (1.0 + jnp.tanh(0.5 * s))
                ).astype(BF16)

    def project_out(l, h, lanes):
        return xs[h, :, lanes].astype(F32) + jnp.dot(wo[l, h], act[:, lanes], preferred_element_type=F32)

    def advance(l, lanes):
        for h in range(2):
            xs[h, :, lanes] = project_out(l, h, lanes).astype(BF16)

    own, outside = slice(BLK, 3 * BLK), slice(0, BLK)

    from_partner(XINN, xs.at[p, :, inn])
    from_partner(XMID, xs.at[p, :, mid])
    normalize(0, (1, 2))
    gate(0, c, own, g1)
    from_partner(WVG, wvg.at[0, p])
    gate(0, p, own, g1)
    inner1 = g1.at[:, :, inn]
    to_outer = remote(FAR, inner1, gfar, (outer, p))

    @pl.when(has_outer)
    def _():
        to_outer.start()

    to_partner(PAR1, inner1, gpar1)
    loaded("wvg1")
    to_partner(WVG + 1, wvg.at[1, c], wvg.at[1, c])
    loaded("wo1")
    to_partner(WO + 1, wo.at[1, c], wo.at[1, c])

    from_partner(TAPS, taps.at[p])
    respond(p)
    from_partner(GG, ggv.at[p])
    from_partner(GS, gsv.at[p])
    spread_groups(p)
    loaded("tables")

    @pl.when(has_outer)
    def _():
        for core in range(2):
            dst = xs.at[(core, *near)]
            pltpu.make_async_remote_copy(
                src_ref=dst, dst_ref=dst, send_sem=ssem.at[NEAR], recv_sem=rsem.at[NEAR + core],
                device_id=(outer, core), device_id_type=MESH,
            ).wait_recv()

    @pl.when(jnp.logical_not(has_outer))
    def _():
        xs[:, :, outside] = jnp.zeros((2, xs.shape[1], BLK), BF16)
        gfar[...] = jnp.zeros_like(gfar)

    normalize(0, (0,))
    for h in range(2):
        gate(0, h, outside, g1)

    from_partner(PAR1, gpar1)
    filter_norm(0, lambda h: jnp.concatenate([g1[h], gpar1[h]], axis=1), slice(0, 2 * BLK), own)
    from_partner(WO, wo.at[0, p])
    advance(0, own)

    normalize(1, (1, 2))
    gate(1, c, own, g2)
    from_partner(WVG + 1, wvg.at[1, p])
    gate(1, p, own, g2)
    to_partner(PAR2, g2.at[:, :, inn], gpar2)

    @pl.when(has_outer)
    def _():
        remote(FAR, gfar, gfar, (outer, p)).wait_recv()

    filter_norm(0, lambda h: jnp.concatenate([gfar[h], g1[h, :, : 2 * BLK]], axis=1), slice(0, BLK), outside)
    advance(0, outside)

    normalize(1, (0,))
    exists = jnp.where(has_outer, 1.0, 0.0)
    for h in range(2):
        gate(1, h, outside, g2, exists)
    from_partner(PAR2, gpar2)
    filter_norm(1, lambda h: jnp.concatenate([g2[h], gpar2[h]], axis=1), slice(0, 2 * BLK), own)
    from_partner(WO + 1, wo.at[1, p])

    obuf[...] = project_out(1, p, own).astype(BF16)
    columns = lambda core: (
        pl.ds(pl.multiple_of(core * 3 * BLK, BLK), BLK),
        pl.ds(pl.multiple_of((1 + core) * BLK, BLK), BLK),
    )
    for k, (lane, b) in enumerate(zip(columns(c), range(2))):
        to_partner(OMID + k, obuf.at[:, pl.ds(b * BLK, BLK)], o_ref.at[:, lane])
    kept = project_out(1, c, own).astype(BF16)
    for lane, b in zip(columns(c), range(2)):
        o_ref[:, lane] = kept[:, b * BLK : (b + 1) * BLK]
    for k, lane in enumerate(columns(p)):
        from_partner(OMID + k, o_ref.at[:, lane])

    for copy in sent:
        copy.wait_send()

    @pl.when(has_left)
    def _():
        to_left.wait_send()

    @pl.when(has_right)
    def _():
        to_right.wait_send()

    @pl.when(has_outer)
    def _():
        to_outer.wait_send()


def solution(mesh):
    n_sp = mesh.shape["sp"]

    def body(stream, norm_gain, w_value, w_gate, conv_taps, group_gain, group_shift, w_out):
        layers, features = norm_gain.shape
        half_features, tokens = stream.shape
        channels = w_value.shape[1]
        taps = conv_taps.shape[2]
        any_spec = pl.BlockSpec(memory_space=pl.ANY)
        vmem = pltpu.VMEM
        return pl.pallas_call(
            functools.partial(kernel, n_sp),
            out_shape=jax.ShapeDtypeStruct(stream.shape, stream.dtype),
            in_specs=[any_spec] * 11,
            out_specs=pl.BlockSpec(memory_space=pltpu.VMEM),
            scratch_shapes=[
                vmem((4, half_features, BLK), BF16),
                vmem((2, half_features, 3 * BLK), BF16),
                vmem((features, 3 * BLK), BF16),
                vmem((layers, 2, 2, 2, BLK, features), BF16),
                vmem((layers, 2, half_features, 2 * channels), BF16),
                vmem((2, layers, channels, taps), BF16),
                vmem((layers, features), F32),
                vmem((2, layers, channels), F32),
                vmem((2, layers, channels), F32),
                vmem((layers, features, BLK), F32),
                vmem((layers, 2, channels, BLK), F32),
                vmem((layers, 2, channels, BLK), F32),
                vmem((layers, 2, channels, SIZE), F32),
                vmem((SIZE, SIZE), BF16),
                vmem((SIZE, 2 * BLK), BF16),
                vmem((taps, SIZE), BF16),
                vmem((2, channels, 3 * BLK), BF16),
                vmem((2, channels, 3 * BLK), BF16),
                vmem((2, channels, BLK), BF16),
                vmem((2, channels, BLK), BF16),
                vmem((2, channels, BLK), BF16),
                vmem((2 * channels, 3 * BLK), BF16),
                vmem((half_features, 2 * BLK), BF16),
                pltpu.SemaphoreType.DMA((21,)),
                pltpu.SemaphoreType.DMA((16,)),
                pltpu.SemaphoreType.DMA((16,)),
            ],
            compiler_params=pltpu.CompilerParams(
                collective_id=0, has_side_effects=True, vmem_limit_bytes=60 * 1024 * 1024
            ),
        )(stream, norm_gain, w_value, w_gate, conv_taps, group_gain, group_shift, w_out, *tables(taps))

    placed = (
        P("tp", "sp"),
        P(),
        P(None, "tp", None),
        P(None, "tp", None),
        P(None, "tp", None),
        P(None, "tp"),
        P(None, "tp"),
        P(None, "tp", None),
    )
    return jax.shard_map(body, mesh=mesh, in_specs=placed, out_specs=P("tp", "sp"), check_vma=False)
```

```python
import functools

import jax
import jax.numpy as jnp
import numpy as np
from jax import lax
from jax.experimental import pallas as pl
from jax.experimental.pallas import tpu as pltpu
from jax.sharding import PartitionSpec as P

MESH = pl.DeviceIdType.MESH
BLK = 128
SIZE = 512
HALF = SIZE // 2
RMS_EPS = 1e-06
LN_EPS = 1e-05
F32 = jnp.float32
BF16 = jnp.bfloat16


def tables(taps):
    angle = lambda t: np.asarray(t)[:, None] * ((np.arange(HALF) + 0.5) * (2 * np.pi / SIZE))[None]
    trig = lambda t: np.concatenate([np.cos(angle(t)), np.sin(angle(t))], axis=1)
    blocks = [np.arange(BLK) + BLK * b for b in range(4)]
    reach = (taps - 1) // 2
    forward = [np.concatenate([trig(blocks[b]) for b in order]) for order in ((0, 1, 2, 3), (3, 2, 1, 0))]
    back = [
        np.concatenate([trig(blocks[b] - reach).T for b in order], axis=1) * (2.0 / SIZE)
        for order in ((1, 2), (2, 1))
    ]
    mixed = np.zeros((2, 2 * BLK, 2, 2 * HALF))
    for layer in range(2):
        mixed[layer, :taps, layer] = trig(np.arange(taps))
    return (
        jnp.asarray(np.stack(forward), BF16),
        jnp.asarray(np.stack(back), BF16),
        jnp.asarray(mixed.reshape(2, 4 * BLK, SIZE), BF16),
    )


def kernel(
    n_sp,
    x_hbm, ng_hbm, wv_hbm, wg_hbm, taps_hbm, gg_hbm, gs_hbm, wo_hbm, fwd_hbm, back_hbm, ftap_hbm,
    o_ref,
    xin, xs, wraw, wvg, wo, taps, ngv, ggv, gsv, ggb, gsb, resp, fwd, back, ftap,
    g1, g2, gfar, gpar1, gpar2, act, obuf,
    lsem, ssem, rsem, ready,
):
    sp, c = lax.axis_index("sp"), lax.axis_index("tp")
    p = 1 - c
    outer = sp + 2 * c - 1
    has_left = sp > 0
    has_right = sp < n_sp - 1
    has_outer = jnp.logical_and(outer >= 0, outer < n_sp)
    left_count = jnp.where(has_left, 1, 0)
    right_count = jnp.where(has_right, 1, 0)
    layers, features = ng_hbm.shape

    barrier = pltpu.get_barrier_semaphore()
    pl.semaphore_signal(barrier, inc=1, device_id=(sp, p), device_id_type=MESH)

    @pl.when(has_outer)
    def _():
        pl.semaphore_signal(barrier, inc=1, device_id=(outer, 1), device_id_type=MESH)

    local, count = {}, [0]

    def load(name, src, dst):
        copy = pltpu.make_async_copy(src, dst, lsem.at[count[0]])
        count[0] += 1
        copy.start()
        local.setdefault(name, []).append(copy)

    def loaded(*names):
        for name in names:
            for copy in local[name]:
                copy.wait()

    def load_wvg(l):
        for k in range(2):
            load(f"w{l}", wv_hbm.at[l, pl.ds(k * BLK, BLK)], wraw.at[l, k, 0])
            load(f"w{l}", wg_hbm.at[l, pl.ds(k * BLK, BLK)], wraw.at[l, k, 1])

    for b in range(4):
        load("x", x_hbm.at[:, pl.ds(b * BLK, BLK)], xin.at[b])
    load("ng", ng_hbm, ngv)
    load_wvg(0)
    load("groups", gg_hbm, ggv.at[c])
    load("groups", gs_hbm, gsv.at[c])
    load("taps", taps_hbm, taps.at[pl.ds(0, taps_hbm.shape[0])])
    load("taps", ftap_hbm, ftap)
    load("tables", fwd_hbm.at[c], fwd)
    load("tables", back_hbm.at[c], back)
    load("wo0", wo_hbm.at[0], wo.at[0, c])
    load_wvg(1)
    load("wo1", wo_hbm.at[1], wo.at[1, c])

    NEAR, FAR, XMID, XINN, WVG, WO, RESP, GG, GS, PAR1, PAR2, OMID = 0, 2, 3, 4, 5, 7, 9, 11, 12, 13, 14, 15
    sent = []

    def remote(k, src, dst, device):
        return pltpu.make_async_remote_copy(
            src_ref=src, dst_ref=dst, send_sem=ssem.at[k], recv_sem=rsem.at[k],
            device_id=device, device_id_type=MESH,
        )

    def to_partner(k, src, dst):
        copy = remote(k, src, dst, (sp, p))
        copy.start()
        sent.append(copy)

    def from_partner(k, dst):
        remote(k, dst, dst, (sp, p)).wait_recv()

    def scale_weights(l):
        gain = ngv[l : l + 1]
        for k in range(2):
            for half in range(2):
                wvg[l, c, k, half] = (wraw[l, k, half].astype(F32) * gain).astype(BF16)

    def spread_groups(h):
        column = lambda row: jnp.broadcast_to(row * 0.5, (BLK, BLK)).T
        for l in range(layers):
            for b in range(2):
                lanes = slice(b * BLK, (b + 1) * BLK)
                ggb[l, h, lanes] = column(ggv[h, l : l + 1, lanes])
                gsb[l, h, lanes] = column(gsv[h, l : l + 1, lanes])

    loaded("x")

    @pl.when(c == 0)
    def _():
        pl.semaphore_wait(barrier, 1)
        pl.semaphore_signal(ready, inc=1, device_id=(sp, 1), device_id_type=MESH)

    @pl.when(c == 1)
    def _():
        pl.semaphore_wait(ready, 1)

    mid, inn = pl.ds(BLK, BLK), pl.ds(2 * BLK, BLK)
    to_partner(XINN, xin.at[1 + p], xs.at[c, :, inn])
    to_partner(XMID, xin.at[3 * p], xs.at[c, :, mid])
    loaded("ng", "w0")
    scale_weights(0)
    loaded("groups")
    to_partner(GG, ggv.at[c], ggv.at[c])
    to_partner(GS, gsv.at[c], gsv.at[c])
    to_partner(WVG, wvg.at[0, c], wvg.at[0, c])

    @pl.when(c == 1)
    def _():
        pl.semaphore_wait(barrier, 1 + left_count + right_count)
        pl.semaphore_signal(ready, inc=1, device_id=(sp, 0), device_id_type=MESH)

    @pl.when(c == 0)
    def _():
        pl.semaphore_wait(ready, 1)

    near = (slice(None), pl.ds(0, BLK))

    def near_copy(b, send, device):
        return pltpu.make_async_remote_copy(
            src_ref=xin.at[b], dst_ref=xs.at[(c, *near)], send_sem=ssem.at[send], recv_sem=rsem.at[NEAR + c],
            device_id=device, device_id_type=MESH,
        )

    to_left = near_copy(0, NEAR, (sp - 1, 1))
    to_right = near_copy(3, NEAR + 1, (sp + 1, 0))

    @pl.when(has_left)
    def _():
        to_left.start()

    @pl.when(has_right)
    def _():
        to_right.start()

    loaded("taps")
    taps[taps_hbm.shape[0] :] = jnp.zeros((taps.shape[0] - taps_hbm.shape[0], *taps.shape[1:]), BF16)
    rows = taps[...].reshape(layers * taps.shape[0], taps.shape[2])
    for l in range(layers):
        resp[l, c] = lax.dot_general(
            rows, ftap[l], (((0,), (0,)), ((), ())), preferred_element_type=F32
        ).astype(BF16)
    spread_groups(c)
    to_partner(RESP, resp.at[0, c], resp.at[0, c])

    xs[c, :, BLK : 2 * BLK] = xin[3 * c]
    xs[c, :, 2 * BLK : 3 * BLK] = xin[1 + c]

    def half_inverse(lanes):
        total = jnp.zeros((1, lanes.stop - lanes.start), F32)
        for h in range(2):
            wide = xs[h, :, lanes].astype(F32)
            total = total + jnp.sum(wide * wide, axis=0, keepdims=True)
        return 0.5 * lax.rsqrt(total * (1.0 / features) + RMS_EPS)

    def gate(l, halves, lanes, dst, inverse, exists=None):
        x = xs[:, :, lanes].reshape(features, lanes.stop - lanes.start)
        kept = inverse if exists is None else inverse * exists
        for h in halves:
            for k in range(2):
                w = wvg[l, h, k].reshape(2 * BLK, features)
                r = jnp.dot(w, x, preferred_element_type=F32)
                value = r[:BLK] * kept
                out = value * jnp.tanh(r[BLK:] * inverse) + value
                dst[h, k * BLK : (k + 1) * BLK, lanes] = out.astype(BF16)

    def filter_norm(l, window, outputs, lanes):
        n = outputs.stop - outputs.start
        for h in range(2):
            w = window(h)
            g = jnp.dot(w, fwd[: w.shape[1]], preferred_element_type=F32)
            gr, gi = g[:, :HALF], g[:, HALF:]
            hr, hi = resp[l, h, :, :HALF].astype(F32), resp[l, h, :, HALF:].astype(F32)
            y = jnp.concatenate([(gr * hr + gi * hi).astype(BF16), (gi * hr - gr * hi).astype(BF16)], axis=1)
            filtered = jnp.dot(y, back[:, outputs], preferred_element_type=F32)
            for k in range(2):
                part = slice(k * BLK, (k + 1) * BLK)
                f = filtered[part]
                centred = f - jnp.sum(f, axis=0, keepdims=True) * (1.0 / BLK)
                variance = jnp.sum(centred * centred, axis=0, keepdims=True) * (1.0 / BLK)
                gain, shift = ggb[l, h, part], gsb[l, h, part]
                if n > BLK:
                    gain = jnp.concatenate([gain] * (n // BLK), axis=1)
                    shift = jnp.concatenate([shift] * (n // BLK), axis=1)
                s = centred * lax.rsqrt(variance + LN_EPS) * gain + shift
                act[h * 2 * BLK + k * BLK : h * 2 * BLK + (k + 1) * BLK, lanes] = (s * jnp.tanh(s) + s).astype(BF16)

    def project_out(l, h, lanes, dst, dst_lanes):
        for half in range(2):
            part = slice(half * 2 * BLK, (half + 1) * 2 * BLK)
            branch = jnp.dot(wo[l, h, part], act[:, lanes], preferred_element_type=F32)
            dst[part, dst_lanes] = (xs[h, part, lanes].astype(F32) + branch).astype(BF16)

    def advance(l, lanes):
        for h in range(2):
            project_out(l, h, lanes, xs.at[h], lanes)

    own, outside = slice(BLK, 3 * BLK), slice(0, BLK)

    from_partner(XINN, xs.at[p, :, inn])
    from_partner(XMID, xs.at[p, :, mid])
    inverse = half_inverse(own)
    gate(0, (c,), own, g1, inverse)
    from_partner(GG, ggv.at[p])
    from_partner(GS, gsv.at[p])
    spread_groups(p)
    from_partner(WVG, wvg.at[0, p])
    gate(0, (p,), own, g1, inverse)
    inner1 = g1.at[:, :, inn]
    to_outer = remote(FAR, inner1, gfar, (outer, p))

    @pl.when(has_outer)
    def _():
        to_outer.start()

    to_partner(PAR1, inner1, gpar1)
    loaded("wo0")
    to_partner(WO, wo.at[0, c], wo.at[0, c])
    loaded("w1")
    scale_weights(1)
    to_partner(WVG + 1, wvg.at[1, c], wvg.at[1, c])
    to_partner(RESP + 1, resp.at[1, c], resp.at[1, c])
    loaded("wo1")
    to_partner(WO + 1, wo.at[1, c], wo.at[1, c])
    loaded("tables")

    @pl.when(has_outer)
    def _():
        for core in range(2):
            dst = xs.at[(core, *near)]
            pltpu.make_async_remote_copy(
                src_ref=dst, dst_ref=dst, send_sem=ssem.at[NEAR], recv_sem=rsem.at[NEAR + core],
                device_id=(outer, core), device_id_type=MESH,
            ).wait_recv()

    @pl.when(jnp.logical_not(has_outer))
    def _():
        xs[:, :, outside] = jnp.zeros((2, xs.shape[1], BLK), BF16)
        gfar[...] = jnp.zeros_like(gfar)

    gate(0, (0, 1), outside, g1, half_inverse(outside))

    from_partner(RESP, resp.at[0, p])
    from_partner(PAR1, gpar1)
    filter_norm(0, lambda h: jnp.concatenate([g1[h], gpar1[h]], axis=1), slice(0, 2 * BLK), own)
    from_partner(WO, wo.at[0, p])
    advance(0, own)

    from_partner(WVG + 1, wvg.at[1, p])
    gate(1, (0, 1), own, g2, half_inverse(own))
    to_partner(PAR2, g2.at[:, :, inn], gpar2)

    @pl.when(has_outer)
    def _():
        remote(FAR, gfar, gfar, (outer, p)).wait_recv()

    filter_norm(0, lambda h: jnp.concatenate([gfar[h], g1[h, :, : 2 * BLK]], axis=1), slice(0, BLK), outside)
    advance(0, outside)

    gate(1, (0, 1), outside, g2, half_inverse(outside), jnp.where(has_outer, 1.0, 0.0))
    from_partner(RESP + 1, resp.at[1, p])
    from_partner(PAR2, gpar2)
    filter_norm(1, lambda h: jnp.concatenate([g2[h], gpar2[h]], axis=1), slice(0, 2 * BLK), own)
    from_partner(WO + 1, wo.at[1, p])

    columns = lambda core: (
        pl.ds(pl.multiple_of(core * 3 * BLK, BLK), BLK),
        pl.ds(pl.multiple_of((1 + core) * BLK, BLK), BLK),
    )
    whole = slice(0, 2 * BLK)
    project_out(1, p, own, obuf.at[0], whole)
    for k, lane in enumerate(columns(c)):
        to_partner(OMID + k, obuf.at[0, :, pl.ds(k * BLK, BLK)], o_ref.at[:, lane])
    project_out(1, c, own, obuf.at[1], whole)
    for k, lane in enumerate(columns(c)):
        o_ref[:, lane] = obuf[1, :, k * BLK : (k + 1) * BLK]
    for k, lane in enumerate(columns(p)):
        from_partner(OMID + k, o_ref.at[:, lane])

    for copy in sent:
        copy.wait_send()

    @pl.when(has_left)
    def _():
        to_left.wait_send()

    @pl.when(has_right)
    def _():
        to_right.wait_send()

    @pl.when(has_outer)
    def _():
        to_outer.wait_send()


def write_kernel(src, dst, sem):
    copy = pltpu.make_async_copy(src, dst, sem)
    copy.start()
    copy.wait()


def write_out(value):
    return pl.pallas_call(
        write_kernel,
        out_shape=jax.ShapeDtypeStruct(value.shape, value.dtype),
        in_specs=[pl.BlockSpec(memory_space=pltpu.VMEM)],
        out_specs=pl.BlockSpec(memory_space=pl.ANY),
        scratch_shapes=[pltpu.SemaphoreType.DMA],
        compiler_params=pltpu.CompilerParams(vmem_limit_bytes=1024 * 1024),
    )(pltpu.with_memory_space_constraint(value, pltpu.VMEM))


def solution(mesh):
    n_sp = mesh.shape["sp"]

    def body(stream, norm_gain, w_value, w_gate, conv_taps, group_gain, group_shift, w_out):
        layers, features = norm_gain.shape
        half_features, tokens = stream.shape
        channels = w_value.shape[1]
        taps = conv_taps.shape[2]
        any_spec = pl.BlockSpec(memory_space=pl.ANY)
        vmem = pltpu.VMEM
        result = pl.pallas_call(
            functools.partial(kernel, n_sp),
            out_shape=pltpu.VMEM(stream.shape, stream.dtype),
            in_specs=[any_spec] * 11,
            out_specs=pl.BlockSpec(memory_space=pltpu.VMEM),
            scratch_shapes=[
                vmem((4, half_features, BLK), BF16),
                vmem((2, half_features, 3 * BLK), BF16),
                vmem((layers, 2, 2, BLK, features), BF16),
                vmem((layers, 2, 2, 2, BLK, features), BF16),
                vmem((layers, 2, half_features, 2 * channels), BF16),
                vmem((2 * BLK, layers, channels), BF16),
                vmem((layers, features), F32),
                vmem((2, layers, channels), F32),
                vmem((2, layers, channels), F32),
                vmem((layers, 2, channels, BLK), F32),
                vmem((layers, 2, channels, BLK), F32),
                vmem((layers, 2, channels, SIZE), BF16),
                vmem((SIZE, SIZE), BF16),
                vmem((SIZE, 2 * BLK), BF16),
                vmem((layers, SIZE, SIZE), BF16),
                vmem((2, channels, 3 * BLK), BF16),
                vmem((2, channels, 3 * BLK), BF16),
                vmem((2, channels, BLK), BF16),
                vmem((2, channels, BLK), BF16),
                vmem((2, channels, BLK), BF16),
                vmem((2 * channels, 3 * BLK), BF16),
                vmem((2, half_features, 2 * BLK), BF16),
                pltpu.SemaphoreType.DMA((21,)),
                pltpu.SemaphoreType.DMA((17,)),
                pltpu.SemaphoreType.DMA((17,)),
                pltpu.SemaphoreType.REGULAR,
            ],
            compiler_params=pltpu.CompilerParams(
                collective_id=0, has_side_effects=True, vmem_limit_bytes=60 * 1024 * 1024
            ),
        )(
            stream, norm_gain, w_value, w_gate, jnp.transpose(conv_taps, (2, 0, 1)),
            group_gain, group_shift, w_out, *tables(taps),
        )
        return write_out(result)

    placed = (
        P("tp", "sp"),
        P(),
        P(None, "tp", None),
        P(None, "tp", None),
        P(None, "tp", None),
        P(None, "tp"),
        P(None, "tp"),
        P(None, "tp", None),
    )
    return jax.shard_map(body, mesh=mesh, in_specs=placed, out_specs=P("tp", "sp"), check_vma=False)
```

```python
import functools

import jax
import jax.numpy as jnp
import numpy as np
from jax import lax
from jax.experimental import pallas as pl
from jax.experimental.pallas import tpu as pltpu
from jax.sharding import PartitionSpec as P

MESH = pl.DeviceIdType.MESH
BLK = 128
SIZE = 512
HALF = SIZE // 2
RMS_EPS = 1e-06
LN_EPS = 1e-05
F32 = jnp.float32
BF16 = jnp.bfloat16


def tables(taps):
    angle = lambda t: np.asarray(t)[:, None] * ((np.arange(HALF) + 0.5) * (2 * np.pi / SIZE))[None]
    trig = lambda t: np.concatenate([np.cos(angle(t)), np.sin(angle(t))], axis=1)
    blocks = [np.arange(BLK) + BLK * b for b in range(4)]
    reach = (taps - 1) // 2
    forward = [np.concatenate([trig(blocks[b]) for b in order]) for order in ((0, 1, 2, 3), (3, 2, 1, 0))]
    back = [
        np.concatenate([trig(blocks[b] - reach).T for b in order], axis=1) * (2.0 / SIZE)
        for order in ((1, 2), (2, 1))
    ]
    mixed = np.zeros((2, 2 * BLK, 2, 2 * HALF))
    for layer in range(2):
        mixed[layer, :taps, layer] = trig(np.arange(taps))
    return (
        jnp.asarray(np.stack(forward), BF16),
        jnp.asarray(np.stack(back), BF16),
        jnp.asarray(mixed.reshape(2, 4 * BLK, SIZE), BF16),
    )


def kernel(
    n_sp,
    x_hbm, ng_hbm, wv_hbm, wg_hbm, taps_hbm, gg_hbm, gs_hbm, wo_hbm, fwd_hbm, back_hbm, ftap_hbm,
    o_ref,
    xin, xs, wraw, wvg, wo, taps, ngv, ggv, gsv, ggb, gsb, resp, fwd, back, ftap,
    g1, g2, gfar, gpar1, gpar2, act, obuf,
    lsem, ssem, rsem, ready,
):
    sp, c = lax.axis_index("sp"), lax.axis_index("tp")
    p = 1 - c
    outer = sp + 2 * c - 1
    has_left = sp > 0
    has_right = sp < n_sp - 1
    has_outer = jnp.logical_and(outer >= 0, outer < n_sp)
    left_count = jnp.where(has_left, 1, 0)
    right_count = jnp.where(has_right, 1, 0)
    layers, features = ng_hbm.shape

    barrier = pltpu.get_barrier_semaphore()
    pl.semaphore_signal(barrier, inc=1, device_id=(sp, p), device_id_type=MESH)

    @pl.when(has_outer)
    def _():
        pl.semaphore_signal(barrier, inc=1, device_id=(outer, 1), device_id_type=MESH)

    local, count = {}, [0]

    def load(name, src, dst):
        copy = pltpu.make_async_copy(src, dst, lsem.at[count[0]])
        count[0] += 1
        copy.start()
        local.setdefault(name, []).append(copy)

    def loaded(*names):
        for name in names:
            for copy in local[name]:
                copy.wait()

    def load_wvg(l):
        for k in range(2):
            load(f"w{l}", wv_hbm.at[l, pl.ds(k * BLK, BLK)], wraw.at[l, k, 0])
            load(f"w{l}", wg_hbm.at[l, pl.ds(k * BLK, BLK)], wraw.at[l, k, 1])

    for b in range(4):
        load("x", x_hbm.at[:, pl.ds(b * BLK, BLK)], xin.at[b])
    load("ng", ng_hbm, ngv)
    load_wvg(0)

    NEAR, FAR, XMID, XINN, WVG, WO, RESP, GG, GS, PAR1, PAR2, OMID = 0, 2, 3, 4, 5, 7, 9, 11, 12, 13, 14, 15
    sent = []

    def remote(k, src, dst, device):
        return pltpu.make_async_remote_copy(
            src_ref=src, dst_ref=dst, send_sem=ssem.at[k], recv_sem=rsem.at[k],
            device_id=device, device_id_type=MESH,
        )

    def to_partner(k, src, dst):
        copy = remote(k, src, dst, (sp, p))
        copy.start()
        sent.append(copy)

    def from_partner(k, dst):
        remote(k, dst, dst, (sp, p)).wait_recv()

    def scale_weights(l):
        gain = ngv[l : l + 1]
        for k in range(2):
            for half in range(2):
                wvg[l, c, k, half] = (wraw[l, k, half].astype(F32) * gain).astype(BF16)

    def spread_groups(h):
        column = lambda row: jnp.broadcast_to(row * 0.5, (BLK, BLK)).T
        for l in range(layers):
            for b in range(2):
                lanes = slice(b * BLK, (b + 1) * BLK)
                ggb[l, h, lanes] = column(ggv[h, l : l + 1, lanes])
                gsb[l, h, lanes] = column(gsv[h, l : l + 1, lanes])

    loaded("x")

    @pl.when(c == 0)
    def _():
        pl.semaphore_wait(barrier, 1)
        pl.semaphore_signal(ready, inc=1, device_id=(sp, 1), device_id_type=MESH)

    @pl.when(c == 1)
    def _():
        pl.semaphore_wait(ready, 1)

    mid, inn = pl.ds(BLK, BLK), pl.ds(2 * BLK, BLK)
    to_partner(XINN, xin.at[1 + p], xs.at[c, :, inn])
    to_partner(XMID, xin.at[3 * p], xs.at[c, :, mid])
    load("groups", gg_hbm, ggv.at[c])
    load("groups", gs_hbm, gsv.at[c])
    load("taps", taps_hbm, taps.at[pl.ds(0, taps_hbm.shape[0])])
    load("taps", ftap_hbm, ftap)
    load("tables", fwd_hbm.at[c], fwd)
    load("tables", back_hbm.at[c], back)
    load("wo0", wo_hbm.at[0], wo.at[0, c])
    load_wvg(1)
    load("wo1", wo_hbm.at[1], wo.at[1, c])
    loaded("ng", "w0")
    scale_weights(0)
    loaded("groups")
    to_partner(GG, ggv.at[c], ggv.at[c])
    to_partner(GS, gsv.at[c], gsv.at[c])
    to_partner(WVG, wvg.at[0, c], wvg.at[0, c])

    @pl.when(c == 1)
    def _():
        pl.semaphore_wait(barrier, 1 + left_count + right_count)
        pl.semaphore_signal(ready, inc=1, device_id=(sp, 0), device_id_type=MESH)

    @pl.when(c == 0)
    def _():
        pl.semaphore_wait(ready, 1)

    near = (slice(None), pl.ds(0, BLK))

    def near_copy(b, send, device):
        return pltpu.make_async_remote_copy(
            src_ref=xin.at[b], dst_ref=xs.at[(c, *near)], send_sem=ssem.at[send], recv_sem=rsem.at[NEAR + c],
            device_id=device, device_id_type=MESH,
        )

    to_left = near_copy(0, NEAR, (sp - 1, 1))
    to_right = near_copy(3, NEAR + 1, (sp + 1, 0))

    @pl.when(has_left)
    def _():
        to_left.start()

    @pl.when(has_right)
    def _():
        to_right.start()

    loaded("taps")
    taps[taps_hbm.shape[0] :] = jnp.zeros((taps.shape[0] - taps_hbm.shape[0], *taps.shape[1:]), BF16)
    rows = taps[...].reshape(layers * taps.shape[0], taps.shape[2])
    for l in range(layers):
        resp[l, c] = lax.dot_general(
            rows, ftap[l], (((0,), (0,)), ((), ())), preferred_element_type=F32
        ).astype(BF16)
    spread_groups(c)
    to_partner(RESP, resp.at[0, c], resp.at[0, c])

    xs[c, :, BLK : 2 * BLK] = xin[3 * c]
    xs[c, :, 2 * BLK : 3 * BLK] = xin[1 + c]

    def half_inverse(lanes):
        total = jnp.zeros((1, lanes.stop - lanes.start), F32)
        for h in range(2):
            wide = xs[h, :, lanes].astype(F32)
            total = total + jnp.sum(wide * wide, axis=0, keepdims=True)
        return 0.5 * lax.rsqrt(total * (1.0 / features) + RMS_EPS)

    def gate(l, halves, lanes, dst, inverse, exists=None):
        x = xs[:, :, lanes].reshape(features, lanes.stop - lanes.start)
        kept = inverse if exists is None else inverse * exists
        for h in halves:
            for k in range(2):
                w = wvg[l, h, k].reshape(2 * BLK, features)
                r = jnp.dot(w, x, preferred_element_type=F32)
                value = r[:BLK] * kept
                out = value * jnp.tanh(r[BLK:] * inverse) + value
                dst[h, k * BLK : (k + 1) * BLK, lanes] = out.astype(BF16)

    def filter_norm(l, window, outputs, lanes):
        n = outputs.stop - outputs.start
        for h in range(2):
            w = window(h)
            g = jnp.dot(w, fwd[: w.shape[1]], preferred_element_type=F32)
            gr, gi = g[:, :HALF], g[:, HALF:]
            hr, hi = resp[l, h, :, :HALF].astype(F32), resp[l, h, :, HALF:].astype(F32)
            y = jnp.concatenate([(gr * hr + gi * hi).astype(BF16), (gi * hr - gr * hi).astype(BF16)], axis=1)
            filtered = jnp.dot(y, back[:, outputs], preferred_element_type=F32)
            for k in range(2):
                part = slice(k * BLK, (k + 1) * BLK)
                f = filtered[part]
                centred = f - jnp.sum(f, axis=0, keepdims=True) * (1.0 / BLK)
                variance = jnp.sum(centred * centred, axis=0, keepdims=True) * (1.0 / BLK)
                gain, shift = ggb[l, h, part], gsb[l, h, part]
                if n > BLK:
                    gain = jnp.concatenate([gain] * (n // BLK), axis=1)
                    shift = jnp.concatenate([shift] * (n // BLK), axis=1)
                s = centred * lax.rsqrt(variance + LN_EPS) * gain + shift
                act[h * 2 * BLK + k * BLK : h * 2 * BLK + (k + 1) * BLK, lanes] = (s * jnp.tanh(s) + s).astype(BF16)

    def project_out(l, h, lanes, dst, dst_lanes):
        for half in range(2):
            part = slice(half * 2 * BLK, (half + 1) * 2 * BLK)
            branch = jnp.dot(wo[l, h, part], act[:, lanes], preferred_element_type=F32)
            dst[part, dst_lanes] = (xs[h, part, lanes].astype(F32) + branch).astype(BF16)

    def advance(l, lanes):
        for h in range(2):
            project_out(l, h, lanes, xs.at[h], lanes)

    own, outside = slice(BLK, 3 * BLK), slice(0, BLK)
    inner, outward = slice(2 * BLK, 3 * BLK), slice(0, 2 * BLK)

    from_partner(XINN, xs.at[p, :, inn])
    from_partner(XMID, xs.at[p, :, mid])
    inverse = half_inverse(own)
    gate(0, (c,), own, g1, inverse)
    from_partner(GG, ggv.at[p])
    from_partner(GS, gsv.at[p])
    spread_groups(p)
    from_partner(WVG, wvg.at[0, p])
    gate(0, (p,), own, g1, inverse)
    inner1 = g1.at[:, :, inn]
    to_outer = remote(FAR, inner1, gfar, (outer, p))

    @pl.when(has_outer)
    def _():
        to_outer.start()

    to_partner(PAR1, inner1, gpar1)
    loaded("wo0")
    to_partner(WO, wo.at[0, c], wo.at[0, c])
    loaded("w1")
    scale_weights(1)
    to_partner(WVG + 1, wvg.at[1, c], wvg.at[1, c])
    to_partner(RESP + 1, resp.at[1, c], resp.at[1, c])
    loaded("wo1")
    to_partner(WO + 1, wo.at[1, c], wo.at[1, c])
    loaded("tables")

    from_partner(RESP, resp.at[0, p])
    from_partner(PAR1, gpar1)
    filter_norm(0, lambda h: jnp.concatenate([g1[h, :, own], gpar1[h]], axis=1), slice(0, BLK), inner)
    from_partner(WO, wo.at[0, p])
    advance(0, inner)
    from_partner(WVG + 1, wvg.at[1, p])
    gate(1, (0, 1), inner, g2, half_inverse(inner))
    to_partner(PAR2, g2.at[:, :, inn], gpar2)

    @pl.when(has_outer)
    def _():
        for core in range(2):
            dst = xs.at[(core, *near)]
            pltpu.make_async_remote_copy(
                src_ref=dst, dst_ref=dst, send_sem=ssem.at[NEAR], recv_sem=rsem.at[NEAR + core],
                device_id=(outer, core), device_id_type=MESH,
            ).wait_recv()

    @pl.when(jnp.logical_not(has_outer))
    def _():
        xs[:, :, outside] = jnp.zeros((2, xs.shape[1], BLK), BF16)
        gfar[...] = jnp.zeros_like(gfar)

    gate(0, (0, 1), outside, g1, half_inverse(outside))

    from_partner(RESP + 1, resp.at[1, p])
    from_partner(WO + 1, wo.at[1, p])
    from_partner(PAR2, gpar2)

    @pl.when(has_outer)
    def _():
        remote(FAR, gfar, gfar, (outer, p)).wait_recv()

    filter_norm(0, lambda h: jnp.concatenate([gfar[h], g1[h]], axis=1), slice(0, 2 * BLK), outward)
    advance(0, outward)
    exists = jnp.where(has_outer, 1.0, 0.0)
    exists = jnp.concatenate([jnp.full((1, BLK), exists, F32), jnp.ones((1, BLK), F32)], axis=1)
    gate(1, (0, 1), outward, g2, half_inverse(outward), exists)
    filter_norm(1, lambda h: jnp.concatenate([g2[h], gpar2[h]], axis=1), slice(0, 2 * BLK), own)

    columns = lambda core: (
        pl.ds(pl.multiple_of(core * 3 * BLK, BLK), BLK),
        pl.ds(pl.multiple_of((1 + core) * BLK, BLK), BLK),
    )
    whole = slice(0, 2 * BLK)
    project_out(1, p, own, obuf.at[0], whole)
    for k, lane in enumerate(columns(c)):
        to_partner(OMID + k, obuf.at[0, :, pl.ds(k * BLK, BLK)], o_ref.at[:, lane])
    project_out(1, c, own, obuf.at[1], whole)
    for k, lane in enumerate(columns(c)):
        o_ref[:, lane] = obuf[1, :, k * BLK : (k + 1) * BLK]
    for k, lane in enumerate(columns(p)):
        from_partner(OMID + k, o_ref.at[:, lane])

    for copy in sent:
        copy.wait_send()

    @pl.when(has_left)
    def _():
        to_left.wait_send()

    @pl.when(has_right)
    def _():
        to_right.wait_send()

    @pl.when(has_outer)
    def _():
        to_outer.wait_send()


def write_kernel(src, dst, sem):
    copy = pltpu.make_async_copy(src, dst, sem)
    copy.start()
    copy.wait()


def write_out(value):
    return pl.pallas_call(
        write_kernel,
        out_shape=jax.ShapeDtypeStruct(value.shape, value.dtype),
        in_specs=[pl.BlockSpec(memory_space=pltpu.VMEM)],
        out_specs=pl.BlockSpec(memory_space=pl.ANY),
        scratch_shapes=[pltpu.SemaphoreType.DMA],
        compiler_params=pltpu.CompilerParams(vmem_limit_bytes=1024 * 1024),
    )(pltpu.with_memory_space_constraint(value, pltpu.VMEM))


def solution(mesh):
    n_sp = mesh.shape["sp"]

    def body(stream, norm_gain, w_value, w_gate, conv_taps, group_gain, group_shift, w_out):
        layers, features = norm_gain.shape
        half_features, tokens = stream.shape
        channels = w_value.shape[1]
        taps = conv_taps.shape[2]
        any_spec = pl.BlockSpec(memory_space=pl.ANY)
        vmem = pltpu.VMEM
        result = pl.pallas_call(
            functools.partial(kernel, n_sp),
            out_shape=pltpu.VMEM(stream.shape, stream.dtype),
            in_specs=[any_spec] * 11,
            out_specs=pl.BlockSpec(memory_space=pltpu.VMEM),
            scratch_shapes=[
                vmem((4, half_features, BLK), BF16),
                vmem((2, half_features, 3 * BLK), BF16),
                vmem((layers, 2, 2, BLK, features), BF16),
                vmem((layers, 2, 2, 2, BLK, features), BF16),
                vmem((layers, 2, half_features, 2 * channels), BF16),
                vmem((2 * BLK, layers, channels), BF16),
                vmem((layers, features), F32),
                vmem((2, layers, channels), F32),
                vmem((2, layers, channels), F32),
                vmem((layers, 2, channels, BLK), F32),
                vmem((layers, 2, channels, BLK), F32),
                vmem((layers, 2, channels, SIZE), BF16),
                vmem((SIZE, SIZE), BF16),
                vmem((SIZE, 2 * BLK), BF16),
                vmem((layers, SIZE, SIZE), BF16),
                vmem((2, channels, 3 * BLK), BF16),
                vmem((2, channels, 3 * BLK), BF16),
                vmem((2, channels, BLK), BF16),
                vmem((2, channels, BLK), BF16),
                vmem((2, channels, BLK), BF16),
                vmem((2 * channels, 3 * BLK), BF16),
                vmem((2, half_features, 2 * BLK), BF16),
                pltpu.SemaphoreType.DMA((21,)),
                pltpu.SemaphoreType.DMA((17,)),
                pltpu.SemaphoreType.DMA((17,)),
                pltpu.SemaphoreType.REGULAR,
            ],
            compiler_params=pltpu.CompilerParams(
                collective_id=0, has_side_effects=True, vmem_limit_bytes=60 * 1024 * 1024
            ),
        )(
            stream, norm_gain, w_value, w_gate, jnp.transpose(conv_taps, (2, 0, 1)),
            group_gain, group_shift, w_out, *tables(taps),
        )
        return write_out(result)

    placed = (
        P("tp", "sp"),
        P(),
        P(None, "tp", None),
        P(None, "tp", None),
        P(None, "tp", None),
        P(None, "tp"),
        P(None, "tp"),
        P(None, "tp", None),
    )
    return jax.shard_map(body, mesh=mesh, in_specs=placed, out_specs=P("tp", "sp"), check_vma=False)
```

```python
import functools

import jax
import jax.numpy as jnp
import numpy as np
from jax import lax
from jax.experimental import pallas as pl
from jax.experimental.pallas import tpu as pltpu
from jax.sharding import PartitionSpec as P

MESH = pl.DeviceIdType.MESH
BLK = 128
SIZE = 512
HALF = SIZE // 2
RMS_EPS = 1e-06
LN_EPS = 1e-05
F32 = jnp.float32
BF16 = jnp.bfloat16


def tables(taps):
    angle = lambda t: np.asarray(t)[:, None] * ((np.arange(HALF) + 0.5) * (2 * np.pi / SIZE))[None]
    trig = lambda t: np.concatenate([np.cos(angle(t)), np.sin(angle(t))], axis=1)
    blocks = [np.arange(BLK) + BLK * b for b in range(4)]
    reach = (taps - 1) // 2
    forward = [np.concatenate([trig(blocks[b]) for b in order]) for order in ((0, 1, 2, 3), (3, 2, 1, 0))]
    back = [
        np.concatenate([trig(blocks[b] - reach).T for b in order], axis=1) * (2.0 / SIZE)
        for order in ((1, 2), (2, 1))
    ]
    mixed = np.zeros((2, 2 * BLK, 2, 2 * HALF))
    for layer in range(2):
        mixed[layer, :taps, layer] = trig(np.arange(taps))
    return (
        jnp.asarray(np.stack(forward), BF16),
        jnp.asarray(np.stack(back), BF16),
        jnp.asarray(mixed.reshape(2, 4 * BLK, SIZE), BF16),
    )


def kernel(
    n_sp,
    x_hbm, ng_hbm, wv_hbm, wg_hbm, taps_hbm, gg_hbm, gs_hbm, wo_hbm, fwd_hbm, back_hbm, ftap_hbm,
    o_ref,
    xall, xs, wraw, wvg, wo, taps, ngv, gv, ggb, gsb, resp, fwd, back, ftap,
    acc, gall, g1, g2, gfar, gpar1, gpar2, act, obuf,
    rsem, ready, lsem, ssem,
):
    sp, c = lax.axis_index("sp"), lax.axis_index("tp")
    p = 1 - c
    outer = sp + 2 * c - 1
    has_left = sp > 0
    has_right = sp < n_sp - 1
    has_outer = jnp.logical_and(outer >= 0, outer < n_sp)
    early = jnp.logical_and(sp == 0, c == 1)
    later = jnp.logical_not(early)
    left_count = jnp.where(has_left, 1, 0)
    right_count = jnp.where(has_right, 1, 0)
    layers, features = ng_hbm.shape

    local = {}

    def load(name, pairs, whole):
        sem = lsem.at[len(local)]
        for src, dst in pairs:
            pltpu.make_async_copy(src, dst, sem).start()
        local[name] = pltpu.make_async_copy(whole, whole, sem)

    def loaded(*names):
        for name in names:
            local[name].wait()

    def load_wvg(l):
        pairs = []
        for k in range(2):
            pairs.append((wv_hbm.at[l, pl.ds(k * BLK, BLK)], wraw.at[l, k, 0]))
            pairs.append((wg_hbm.at[l, pl.ds(k * BLK, BLK)], wraw.at[l, k, 1]))
        load(f"w{l}", pairs, wraw.at[l])

    load("x", [(x_hbm.at[:, pl.ds(b * BLK, BLK)], xall.at[c, b]) for b in range(4)], xall.at[c])

    barrier = pltpu.get_barrier_semaphore()
    pl.semaphore_signal(barrier, inc=1, device_id=(sp, p), device_id_type=MESH)

    @pl.when(has_outer)
    def _():
        pl.semaphore_signal(barrier, inc=1, device_id=(outer, 1), device_id_type=MESH)

    load("ng", [(ng_hbm, ngv)], ngv)
    load_wvg(0)
    load("groups", [(gg_hbm, gv.at[c, 0]), (gs_hbm, gv.at[c, 1])], gv.at[c])
    load("wo0", [(wo_hbm.at[0], wo.at[0, c])], wo.at[0, c])
    tap_rows = taps.at[pl.ds(0, taps_hbm.shape[0])]
    load("taps", [(taps_hbm, tap_rows)], tap_rows)
    load("ftap", [(ftap_hbm, ftap)], ftap)
    load_wvg(1)
    load("fwd", [(fwd_hbm.at[c], fwd)], fwd)
    load("back", [(back_hbm.at[c], back)], back)
    load("wo1", [(wo_hbm.at[1], wo.at[1, c])], wo.at[1, c])

    NEAR, FAR, X, GMID, GINN, WVG, WO, RESP, GV, PAR1, PAR2, OMID = 0, 2, 4, 5, 6, 7, 10, 12, 14, 15, 16, 17
    sent = []

    def remote(k, src, dst, device):
        return pltpu.make_async_remote_copy(
            src_ref=src, dst_ref=dst, send_sem=ssem.at[k], recv_sem=rsem.at[k],
            device_id=device, device_id_type=MESH,
        )

    def to_partner(k, src, dst, when=None):
        copy = remote(k, src, dst, (sp, p))
        if when is None:
            copy.start()
        else:
            pl.when(when)(copy.start)
        if when is not later:
            sent.append(copy)

    def share(ref, k, l, when=None):
        to_partner(k + l, ref.at[l, c], ref.at[l, c], when)

    def from_partner(k, dst):
        remote(k, dst, dst, (sp, p)).wait_recv()

    def to_neighbour(first, direction, src, dst):
        return pltpu.make_async_remote_copy(
            src_ref=src, dst_ref=dst, send_sem=ssem.at[first + direction], recv_sem=rsem.at[first + c],
            device_id=(sp + 2 * direction - 1, 1 - direction), device_id_type=MESH,
        )

    def from_outer(first, part):
        for core in range(2):
            dst = part(core)
            pltpu.make_async_remote_copy(
                src_ref=dst, dst_ref=dst, send_sem=ssem.at[first], recv_sem=rsem.at[first + core],
                device_id=(outer, core), device_id_type=MESH,
            ).wait_recv()

    def start_both(copies):
        for there, copy in zip((has_left, has_right), copies):
            pl.when(there)(copy.start)

    def scale_weights(l):
        gain = ngv[l : l + 1]
        for k in range(2):
            for half in range(2):
                wvg[l, c, k, half] = (wraw[l, k, half].astype(F32) * gain).astype(BF16)

    def spread_groups(h):
        column = lambda row: jnp.broadcast_to(row * 0.5, (BLK, BLK)).T
        for l in range(layers):
            for b in range(2):
                lanes = slice(b * BLK, (b + 1) * BLK)
                ggb[l, h, lanes] = column(gv[h, 0, l : l + 1, lanes])
                gsb[l, h, lanes] = column(gv[h, 1, l : l + 1, lanes])

    def prepare_gates():
        loaded("groups", "ng", "w0")
        scale_weights(0)

    def prepare_taps():
        loaded("taps", "ftap")
        taps[taps_hbm.shape[0] :] = jnp.zeros((taps.shape[0] - taps_hbm.shape[0], *taps.shape[1:]), BF16)

    def respond(l):
        rows = taps[...].reshape(layers * taps.shape[0], taps.shape[2])
        resp[l, c] = lax.dot_general(
            rows, ftap[l], (((0,), (0,)), ((), ())), preferred_element_type=F32
        ).astype(BF16)

    def prepare_weights():
        loaded("w1")
        scale_weights(1)

    @pl.when(early)
    def _():
        prepare_gates()
        prepare_taps()
        for l in range(layers):
            respond(l)
        prepare_weights()
        spread_groups(c)

    @pl.when(c == 0)
    def _():
        pl.semaphore_wait(barrier, 1)
        pl.semaphore_signal(ready, inc=1, device_id=(sp, 1), device_id_type=MESH)

    @pl.when(c == 1)
    def _():
        pl.semaphore_wait(ready, 1)

    loaded("x")
    to_partner(X, xall.at[c], xall.at[c])

    @pl.when(c == 1)
    def _():
        pl.semaphore_wait(barrier, 1 + left_count + right_count)
        pl.semaphore_signal(ready, inc=1, device_id=(sp, 0), device_id_type=MESH)

    @pl.when(c == 0)
    def _():
        pl.semaphore_wait(ready, 1)

    near = (slice(None), pl.ds(0, BLK))
    near_copies = [to_neighbour(NEAR, d, xall.at[c, 3 * d], xs.at[(c, *near)]) for d in range(2)]
    start_both(near_copies)

    pl.when(later)(prepare_gates)
    to_partner(GV, gv.at[c], gv.at[c])
    loaded("wo0")
    share(wo, WO, 0)
    for l in range(layers):
        share(resp, RESP, l, early)

    def squares(x):
        wide = x.astype(F32)
        return jnp.sum(wide * wide, axis=0, keepdims=True)

    def half_inverse(total):
        return 0.5 * lax.rsqrt(total * (1.0 / features) + RMS_EPS)

    def gated(r, inverse, kept):
        value = r[:BLK] * kept
        return (value * jnp.tanh(r[BLK:] * inverse) + value).astype(BF16)

    def gate(l, lanes, dst, exists=None, arrived=None):
        x = xs[:, :, lanes].reshape(features, lanes.stop - lanes.start)
        inverse = half_inverse(squares(x))
        kept = inverse if exists is None else inverse * exists
        for h in range(2) if arrived is None else (c, p):
            if h is p:
                arrived()
            for k in range(2):
                r = jnp.dot(wvg[l, h, k].reshape(2 * BLK, features), x, preferred_element_type=F32)
                dst[h, k * BLK : (k + 1) * BLK, lanes] = gated(r, inverse, kept)

    def filter_norm(l, window, outputs, lanes, halves=(0, 1)):
        n = outputs.stop - outputs.start
        for h in halves:
            w = window(h)
            g = jnp.dot(w, fwd[: w.shape[1]], preferred_element_type=F32)
            gr, gi = g[:, :HALF], g[:, HALF:]
            hr, hi = resp[l, h, :, :HALF].astype(F32), resp[l, h, :, HALF:].astype(F32)
            y = jnp.concatenate([(gr * hr + gi * hi).astype(BF16), (gi * hr - gr * hi).astype(BF16)], axis=1)
            filtered = jnp.dot(y, back[:, outputs], preferred_element_type=F32)
            for k in range(2):
                part = slice(k * BLK, (k + 1) * BLK)
                f = filtered[part]
                centred = f - jnp.sum(f, axis=0, keepdims=True) * (1.0 / BLK)
                variance = jnp.sum(centred * centred, axis=0, keepdims=True) * (1.0 / BLK)
                gain, shift = ggb[l, h, part], gsb[l, h, part]
                if n > BLK:
                    gain = jnp.concatenate([gain] * (n // BLK), axis=1)
                    shift = jnp.concatenate([shift] * (n // BLK), axis=1)
                s = centred * lax.rsqrt(variance + LN_EPS) * gain + shift
                act[h, part, lanes] = (s * jnp.tanh(s) + s).astype(BF16)

    def project_out(l, h, lanes, dst, dst_lanes, pieces=((0, 2 * BLK), (2 * BLK, 2 * BLK))):
        for first, size in pieces:
            part = slice(first, first + size)
            activated = act[:, :, lanes].reshape(wo.shape[3], lanes.stop - lanes.start)
            branch = jnp.dot(wo[l, h, part], activated, preferred_element_type=F32)
            dst[part, dst_lanes] = (xs[h, part, lanes].astype(F32) + branch).astype(BF16)

    def advance(l, lanes):
        for h in range(2):
            project_out(l, h, lanes, xs.at[h], lanes)

    own, outside = slice(BLK, 3 * BLK), slice(0, BLK)
    inner, outward = slice(2 * BLK, 3 * BLK), slice(0, 2 * BLK)

    part_rows = features // 2

    def part_dot(core, k):
        x = jnp.concatenate([xall[core, b] for b in range(4)], axis=1)
        w = wvg[0, c, k, :, :, pl.ds(pl.multiple_of(core * part_rows, part_rows), part_rows)]
        return jnp.dot(w.reshape(2 * BLK, part_rows), x, preferred_element_type=F32)

    def part_squares(core):
        return jnp.concatenate([squares(xall[core, b]) for b in range(4)], axis=1)

    for k in range(2):
        acc[k] = part_dot(c, k)
    total = part_squares(c)
    from_partner(X, xall.at[p])
    inverse = half_inverse(total + part_squares(p))
    for k in range(2):
        gk = gated(acc[k] + part_dot(p, k), inverse, inverse)
        for b in range(4):
            gall[b, k * BLK : (k + 1) * BLK] = gk[:, b * BLK : (b + 1) * BLK]
    mid, inn = pl.ds(BLK, BLK), pl.ds(2 * BLK, BLK)
    to_partner(GINN, gall.at[1 + p], g1.at[c, :, inn])
    to_partner(PAR1, gall.at[1 + c], gpar1.at[c])
    to_partner(GMID, gall.at[3 * p], g1.at[c, :, mid])
    far_copies = [to_neighbour(FAR, d, gall.at[1 + d], gfar.at[c]) for d in range(2)]
    start_both(far_copies)

    @pl.when(later)
    def _():
        prepare_taps()
        respond(0)

    share(resp, RESP, 0, later)
    pl.when(later)(prepare_weights)
    share(wvg, WVG, 1)
    share(wvg, WVG, 0)
    for h in range(2):
        xs[h, :, BLK : 2 * BLK] = xall[h, 3 * c]
        xs[h, :, 2 * BLK : 3 * BLK] = xall[h, 1 + c]
    g1[c, :, BLK : 2 * BLK] = gall[3 * c]
    g1[c, :, 2 * BLK : 3 * BLK] = gall[1 + c]
    gpar1[c] = gall[1 + p]

    loaded("fwd", "back")

    @pl.when(later)
    def _():
        spread_groups(c)

    inner_window = lambda h: jnp.concatenate([g1[h, :, own], gpar1[h]], axis=1)
    filter_norm(0, inner_window, slice(0, BLK), inner, (c,))
    from_partner(GV, gv.at[p])
    spread_groups(p)

    from_partner(RESP, resp.at[0, p])
    from_partner(WO, wo.at[0, p])
    from_partner(GINN, g1.at[p, :, inn])
    from_partner(PAR1, gpar1.at[p])
    from_partner(GMID, g1.at[p, :, mid])
    filter_norm(0, inner_window, slice(0, BLK), inner, (p,))
    advance(0, inner)
    from_partner(WVG + 1, wvg.at[1, p])
    gate(1, inner, g2)
    to_partner(PAR2, g2.at[:, :, inn], gpar2)
    pl.when(later)(lambda: respond(1))
    share(resp, RESP, 1, later)
    loaded("wo1")
    share(wo, WO, 1)

    @pl.when(has_outer)
    def _():
        from_outer(NEAR, lambda core: xs.at[(core, *near)])
        gate(0, outside, g1, arrived=lambda: from_partner(WVG, wvg.at[0, p]))

    @pl.when(jnp.logical_not(has_outer))
    def _():
        from_partner(WVG, wvg.at[0, p])
        xs[:, :, outside] = jnp.zeros((2, xs.shape[1], BLK), BF16)
        g1[:, :, outside] = jnp.zeros_like(gfar)
        gfar[...] = jnp.zeros_like(gfar)

    @pl.when(has_outer)
    def _():
        from_outer(FAR, lambda core: gfar.at[core])

    filter_norm(0, lambda h: jnp.concatenate([gfar[h], g1[h]], axis=1), slice(0, 2 * BLK), outward)
    advance(0, outward)
    exists = jnp.where(has_outer, 1.0, 0.0)
    gate(1, outward, g2, jnp.concatenate([jnp.full((1, BLK), exists, F32), jnp.ones((1, BLK), F32)], axis=1))
    from_partner(PAR2, gpar2)
    from_partner(RESP + 1, resp.at[1, p])
    from_partner(WO + 1, wo.at[1, p])
    filter_norm(1, lambda h: jnp.concatenate([g2[h], gpar2[h]], axis=1), slice(0, 2 * BLK), own)

    columns = lambda core: (
        pl.ds(pl.multiple_of(core * 3 * BLK, BLK), BLK),
        pl.ds(pl.multiple_of((1 + core) * BLK, BLK), BLK),
    )
    whole = slice(0, 2 * BLK)
    pairs = [tuple((2 * q * BLK + r * BLK, BLK) for r in range(2)) for q in range(2)]
    for q in range(2):
        project_out(1, p, own, obuf.at[0], whole, pairs[q])
        part = pl.ds(2 * q * BLK, 2 * BLK)
        for k, lane in enumerate(columns(c)):
            to_partner(OMID + 2 * q + k, obuf.at[0, part, pl.ds(k * BLK, BLK)], o_ref.at[part, lane])
    project_out(1, c, own, obuf.at[1], whole)
    for k, lane in enumerate(columns(c)):
        o_ref[:, lane] = obuf[1, :, k * BLK : (k + 1) * BLK]
    for copies in (near_copies, far_copies):
        for there, copy in zip((has_left, has_right), copies):
            pl.when(there)(copy.wait_send)
    for copy in sent:
        copy.wait_send()
    for q in range(2):
        part = pl.ds(2 * q * BLK, 2 * BLK)
        for k, lane in enumerate(columns(p)):
            from_partner(OMID + 2 * q + k, o_ref.at[part, lane])


def scoped(n_sp, *refs):
    pl.run_scoped(
        lambda *semaphores: kernel(n_sp, *refs, *semaphores),
        pltpu.SemaphoreType.DMA((11,)),
        pltpu.SemaphoreType.DMA((21,)),
    )


def write_kernel(src, dst, sem):
    copy = pltpu.make_async_copy(src, dst, sem)
    copy.start()
    copy.wait()


def write_out(value):
    return pl.pallas_call(
        write_kernel,
        out_shape=jax.ShapeDtypeStruct(value.shape, value.dtype),
        in_specs=[pl.BlockSpec(memory_space=pltpu.VMEM)],
        out_specs=pl.BlockSpec(memory_space=pl.ANY),
        scratch_shapes=[pltpu.SemaphoreType.DMA],
        compiler_params=pltpu.CompilerParams(vmem_limit_bytes=1024 * 1024),
    )(pltpu.with_memory_space_constraint(value, pltpu.VMEM))


def solution(mesh):
    n_sp = mesh.shape["sp"]

    def body(stream, norm_gain, w_value, w_gate, conv_taps, group_gain, group_shift, w_out):
        layers, features = norm_gain.shape
        half_features, tokens = stream.shape
        channels = w_value.shape[1]
        taps = conv_taps.shape[2]
        any_spec = pl.BlockSpec(memory_space=pl.ANY)
        vmem = pltpu.VMEM
        result = pl.pallas_call(
            functools.partial(scoped, n_sp),
            out_shape=pltpu.VMEM(stream.shape, stream.dtype),
            in_specs=[any_spec] * 11,
            out_specs=pl.BlockSpec(memory_space=pltpu.VMEM),
            scratch_shapes=[
                vmem((2, 4, half_features, BLK), BF16),
                vmem((2, half_features, 3 * BLK), BF16),
                vmem((layers, 2, 2, BLK, features), BF16),
                vmem((layers, 2, 2, 2, BLK, features), BF16),
                vmem((layers, 2, half_features, 2 * channels), BF16),
                vmem((2 * BLK, layers, channels), BF16),
                vmem((layers, features), F32),
                vmem((2, 2, layers, channels), F32),
                vmem((layers, 2, channels, BLK), F32),
                vmem((layers, 2, channels, BLK), F32),
                vmem((layers, 2, channels, SIZE), BF16),
                vmem((SIZE, SIZE), BF16),
                vmem((SIZE, 2 * BLK), BF16),
                vmem((layers, SIZE, SIZE), BF16),
                vmem((2, 2 * BLK, tokens), F32),
                vmem((4, channels, BLK), BF16),
                vmem((2, channels, 3 * BLK), BF16),
                vmem((2, channels, 3 * BLK), BF16),
                vmem((2, channels, BLK), BF16),
                vmem((2, channels, BLK), BF16),
                vmem((2, channels, BLK), BF16),
                vmem((2, channels, 3 * BLK), BF16),
                vmem((2, half_features, 2 * BLK), BF16),
                pltpu.SemaphoreType.DMA((21,)),
                pltpu.SemaphoreType.REGULAR,
            ],
            compiler_params=pltpu.CompilerParams(
                collective_id=0, has_side_effects=True, vmem_limit_bytes=60 * 1024 * 1024
            ),
        )(
            stream, norm_gain, w_value, w_gate, jnp.transpose(conv_taps, (2, 0, 1)),
            group_gain, group_shift, w_out, *tables(taps),
        )
        return write_out(result)

    placed = (
        P("tp", "sp"),
        P(),
        P(None, "tp", None),
        P(None, "tp", None),
        P(None, "tp", None),
        P(None, "tp"),
        P(None, "tp"),
        P(None, "tp", None),
    )
    return jax.shard_map(body, mesh=mesh, in_specs=placed, out_specs=P("tp", "sp"), check_vma=False)
```

```python
import functools

import jax
import jax.numpy as jnp
import numpy as np
from jax import lax
from jax.experimental import pallas as pl
from jax.experimental.pallas import tpu as pltpu
from jax.sharding import PartitionSpec as P

MESH = pl.DeviceIdType.MESH
BLK = 128
SIZE = 512
HALF = SIZE // 2
RMS_EPS = 1e-06
LN_EPS = 1e-05
F32 = jnp.float32
BF16 = jnp.bfloat16


def tables(taps):
    angle = lambda t: np.asarray(t)[:, None] * ((np.arange(HALF) + 0.5) * (2 * np.pi / SIZE))[None]
    trig = lambda t: np.stack([np.cos(angle(t)), np.sin(angle(t))], axis=1).reshape(
        -1, 2, 2, BLK
    ).transpose(0, 2, 1, 3).reshape(-1, SIZE)
    blocks = [np.arange(BLK) + BLK * b for b in range(4)]
    reach = (taps - 1) // 2
    forward = [np.concatenate([trig(blocks[b]) for b in order]) for order in ((0, 1, 2, 3), (3, 2, 1, 0))]
    back = [
        np.concatenate([trig(blocks[b] - reach).T for b in order], axis=1) * (2.0 / SIZE)
        for order in ((1, 2), (2, 1))
    ]
    mixed = np.zeros((2, 2 * BLK, 2, 2 * HALF))
    for layer in range(2):
        mixed[layer, :taps, layer] = trig(np.arange(taps))
    return (
        jnp.asarray(np.stack(forward), BF16),
        jnp.asarray(np.stack(back), BF16),
        jnp.asarray(mixed.reshape(2, 4 * BLK, SIZE), BF16),
    )


def kernel(
    n_sp,
    x_hbm, ng_hbm, wv_hbm, wg_hbm, taps_hbm, gg_hbm, gs_hbm, wo_hbm, fwd_hbm, back_hbm, ftap_hbm,
    o_ref,
    xall, xs, wraw, wvg, wo, taps, ngv, gv, ggb, gsb, resp, fwd, back, ftap,
    acc, gall, g1, g2, gfar, gnear, gpar1, gpar2, act, obuf,
    rsem, ready, lsem, ssem,
):
    sp, c = lax.axis_index("sp"), lax.axis_index("tp")
    p = 1 - c
    outer = sp + 2 * c - 1
    has_left = sp > 0
    has_right = sp < n_sp - 1
    has_outer = jnp.logical_and(outer >= 0, outer < n_sp)
    first = sp == 0
    head = jnp.logical_and(first, c == 0)
    early = jnp.logical_and(first, c == 1)
    later = jnp.logical_not(early)
    past = sp > 0
    left_count = jnp.where(has_left, 1, 0)
    right_count = jnp.where(has_right, 1, 0)
    layers, features = ng_hbm.shape

    local = {}

    def load(name, pairs, whole):
        sem = lsem.at[len(local)]
        for src, dst in pairs:
            pltpu.make_async_copy(src, dst, sem).start()
        local[name] = pltpu.make_async_copy(whole, whole, sem)

    def loaded(*names):
        for name in names:
            local[name].wait()

    def load_wvg(l):
        pairs = []
        for k in range(2):
            pairs.append((wv_hbm.at[l, pl.ds(k * BLK, BLK)], wraw.at[l, k, 0]))
            pairs.append((wg_hbm.at[l, pl.ds(k * BLK, BLK)], wraw.at[l, k, 1]))
        load(f"w{l}", pairs, wraw.at[l])

    load("x", [(x_hbm.at[:, pl.ds(b * BLK, BLK)], xall.at[c, b]) for b in range(4)], xall.at[c])

    barrier = pltpu.get_barrier_semaphore()
    pl.semaphore_signal(barrier, inc=1, device_id=(sp, p), device_id_type=MESH)

    @pl.when(has_outer)
    def _():
        pl.semaphore_signal(barrier, inc=1, device_id=(outer, 1), device_id_type=MESH)

    load("ng", [(ng_hbm, ngv)], ngv)
    load("groups", [(gg_hbm, gv.at[c, 0]), (gs_hbm, gv.at[c, 1])], gv.at[c])
    load_wvg(0)
    load("wo0", [(wo_hbm.at[0], wo.at[0, c])], wo.at[0, c])
    tap_rows = taps.at[pl.ds(0, taps_hbm.shape[0])]
    load("taps", [(taps_hbm, tap_rows)], tap_rows)
    load("ftap", [(ftap_hbm, ftap)], ftap)
    load_wvg(1)
    load("fwd", [(fwd_hbm.at[c], fwd)], fwd)
    load("back", [(back_hbm.at[c], back)], back)
    load("wo1", [(wo_hbm.at[1], wo.at[1, c])], wo.at[1, c])

    NEAR, FAR, X, GMID, GINN, WVG, WO, RESP, GV, PAR1, PAR2, OMID = 0, 2, 4, 5, 6, 7, 9, 11, 13, 14, 15, 16
    FORTH, BACK = 20, 21
    sent = []

    def remote(k, src, dst, device):
        return pltpu.make_async_remote_copy(
            src_ref=src, dst_ref=dst, send_sem=ssem.at[k], recv_sem=rsem.at[k],
            device_id=device, device_id_type=MESH,
        )

    def to_partner(k, src, dst, when=None):
        copy = remote(k, src, dst, (sp, p))
        if when is None:
            copy.start()
        else:
            pl.when(when)(copy.start)
        if when is not later:
            sent.append((None if when is early else when, copy))

    def share(ref, k, l, when=None):
        to_partner(k + l, ref.at[l, c], ref.at[l, c], when)

    def from_partner(k, dst):
        remote(k, dst, dst, (sp, p)).wait_recv()

    def to_neighbour(first, direction, src, dst):
        return pltpu.make_async_remote_copy(
            src_ref=src, dst_ref=dst, send_sem=ssem.at[first + direction], recv_sem=rsem.at[first + c],
            device_id=(sp + 2 * direction - 1, 1 - direction), device_id_type=MESH,
        )

    def from_outer(first, part):
        for core in range(2):
            dst = part(core)
            pltpu.make_async_remote_copy(
                src_ref=dst, dst_ref=dst, send_sem=ssem.at[first], recv_sem=rsem.at[first + core],
                device_id=(outer, core), device_id_type=MESH,
            ).wait_recv()

    def start_both(copies):
        for there, copy in zip((has_left, has_right), copies):
            pl.when(there)(copy.start)

    def scale_weights(l):
        gain = ngv[l : l + 1]
        for k in range(2):
            for half in range(2):
                wvg[l, c, k, half] = (wraw[l, k, half].astype(F32) * gain).astype(BF16)

    def spread_groups(h):
        column = lambda row: jnp.broadcast_to(row * 0.5, (BLK, BLK)).T
        for l in range(layers):
            for b in range(2):
                lanes = slice(b * BLK, (b + 1) * BLK)
                ggb[l, h, lanes] = column(gv[h, 0, l : l + 1, lanes])
                gsb[l, h, lanes] = column(gv[h, 1, l : l + 1, lanes])

    def prepare_gates():
        loaded("groups")
        spread_groups(c)
        loaded("ng", "w0")
        scale_weights(0)

    def prepare_taps():
        loaded("taps", "ftap")
        taps[taps_hbm.shape[0] :] = jnp.zeros((taps.shape[0] - taps_hbm.shape[0], *taps.shape[1:]), BF16)

    def respond(l):
        rows = taps[...].reshape(layers * taps.shape[0], taps.shape[2])
        resp[l, c] = lax.dot_general(
            rows, ftap[l], (((0,), (0,)), ((), ())), preferred_element_type=F32
        ).astype(BF16)

    def prepare_weights():
        loaded("w1")
        scale_weights(1)

    @pl.when(early)
    def _():
        prepare_gates()
        prepare_taps()
        for l in range(layers):
            respond(l)
        prepare_weights()

    @pl.when(c == 0)
    def _():
        pl.semaphore_wait(barrier, 1)
        pl.semaphore_signal(ready, inc=1, device_id=(sp, 1), device_id_type=MESH)

    @pl.when(c == 1)
    def _():
        pl.semaphore_wait(ready, 1)

    loaded("x")
    to_partner(X, xall.at[c], xall.at[c])

    @pl.when(c == 1)
    def _():
        pl.semaphore_wait(barrier, 1 + left_count + right_count)
        pl.semaphore_signal(ready, inc=1, device_id=(sp, 0), device_id_type=MESH)

    @pl.when(c == 0)
    def _():
        pl.semaphore_wait(ready, 1)

    near = (slice(None), pl.ds(0, BLK))
    near_copies = [to_neighbour(NEAR, d, xall.at[c, 3 * d], xs.at[(c, *near)]) for d in range(2)]
    start_both(near_copies)

    pl.when(later)(prepare_gates)
    to_partner(GV, gv.at[c], gv.at[c])
    loaded("wo0")
    share(wo, WO, 0)
    for l in range(layers):
        share(resp, RESP, l, early)

    def squares(x):
        wide = x.astype(F32)
        return jnp.sum(wide * wide, axis=0, keepdims=True)

    def half_inverse(total):
        return 0.5 * lax.rsqrt(total * (1.0 / features) + RMS_EPS)

    def gated(r, inverse, kept):
        value = r[:BLK] * kept
        return (value * jnp.tanh(r[BLK:] * inverse) + value).astype(BF16)

    def gate(l, lanes, dst, exists=None, arrived=None, halves=(0, 1)):
        x = xs[:, :, lanes].reshape(features, lanes.stop - lanes.start)
        inverse = half_inverse(squares(x))
        kept = inverse if exists is None else inverse * exists
        for h in halves if arrived is None else (c, p):
            if h is p:
                arrived()
            for k in range(2):
                r = jnp.dot(wvg[l, h, k].reshape(2 * BLK, features), x, preferred_element_type=F32)
                dst[h, k * BLK : (k + 1) * BLK, lanes] = gated(r, inverse, kept)

    def filter_norm(l, window, outputs, lanes, halves=(0, 1)):
        n = outputs.stop - outputs.start
        for h in halves:
            w = window(h)
            filtered = None
            for q in range(2):
                both, re, im = (slice(2 * q * BLK + i * BLK, 2 * q * BLK + j * BLK) for i, j in ((0, 2), (0, 1), (1, 2)))
                g = jnp.dot(w, fwd[: w.shape[1], both], preferred_element_type=F32)
                gr, gi = g[:, :BLK], g[:, BLK:]
                hr, hi = resp[l, h, :, re].astype(F32), resp[l, h, :, im].astype(F32)
                y = jnp.concatenate([(gr * hr + gi * hi).astype(BF16), (gi * hr - gr * hi).astype(BF16)], axis=1)
                term = jnp.dot(y, back[both, outputs], preferred_element_type=F32)
                filtered = term if filtered is None else filtered + term
            for k in range(2):
                part = slice(k * BLK, (k + 1) * BLK)
                f = filtered[part]
                centred = f - jnp.sum(f, axis=0, keepdims=True) * (1.0 / BLK)
                variance = jnp.sum(centred * centred, axis=0, keepdims=True) * (1.0 / BLK)
                gain, shift = ggb[l, h, part], gsb[l, h, part]
                if n > BLK:
                    gain = jnp.concatenate([gain] * (n // BLK), axis=1)
                    shift = jnp.concatenate([shift] * (n // BLK), axis=1)
                s = centred * lax.rsqrt(variance + LN_EPS) * gain + shift
                act[h, part, lanes] = (s * jnp.tanh(s) + s).astype(BF16)

    def project_out(l, h, lanes, dst, dst_lanes, pieces=((0, 2 * BLK), (2 * BLK, 2 * BLK))):
        for first, size in pieces:
            part = slice(first, first + size)
            activated = act[:, :, lanes].reshape(wo.shape[3], lanes.stop - lanes.start)
            branch = jnp.dot(wo[l, h, part], activated, preferred_element_type=F32)
            dst[part, dst_lanes] = (xs[h, part, lanes].astype(F32) + branch).astype(BF16)

    def advance(l, lanes):
        for h in range(2):
            project_out(l, h, lanes, xs.at[h], lanes)

    own, outside = slice(BLK, 3 * BLK), slice(0, BLK)
    inner, outward = slice(2 * BLK, 3 * BLK), slice(0, 2 * BLK)

    part_rows = features // 2

    def part_dot(core, k):
        x = jnp.concatenate([xall[core, b] for b in range(4)], axis=1)
        w = wvg[0, c, k, :, :, pl.ds(pl.multiple_of(core * part_rows, part_rows), part_rows)]
        return jnp.dot(w.reshape(2 * BLK, part_rows), x, preferred_element_type=F32)

    def part_squares(core):
        return jnp.concatenate([squares(xall[core, b]) for b in range(4)], axis=1)

    for k in range(2):
        acc[k] = part_dot(c, k)
    total = part_squares(c)
    near_block = xs.at[(slice(None), *near)]
    forth = remote(FORTH, near_block, near_block, (sp, p))
    back_again = remote(BACK, gnear.at[c], g1.at[(c, *near)], (sp, p))

    @pl.when(early)
    def _():
        from_outer(NEAR, lambda core: xs.at[(core, *near)])
        forth.start()
        gate(0, outside, g1, halves=(c,))

    from_partner(X, xall.at[p])
    inverse = half_inverse(total + part_squares(p))
    for k in range(2):
        gk = gated(acc[k] + part_dot(p, k), inverse, inverse)
        for b in range(4):
            gall[b, k * BLK : (k + 1) * BLK] = gk[:, b * BLK : (b + 1) * BLK]
    mid, inn = pl.ds(BLK, BLK), pl.ds(2 * BLK, BLK)
    to_partner(GINN, gall.at[1 + p], g1.at[c, :, inn])
    to_partner(PAR1, gall.at[1 + c], gpar1.at[c])
    to_partner(GMID, gall.at[3 * p], g1.at[c, :, mid])
    far_copies = [to_neighbour(FAR, d, gall.at[1 + d], gfar.at[c]) for d in range(2)]
    start_both(far_copies)

    @pl.when(later)
    def _():
        prepare_taps()
        respond(0)

    share(resp, RESP, 0, later)
    pl.when(later)(prepare_weights)
    share(wvg, WVG, 1)
    share(wvg, WVG, 0, past)
    for h in range(2):
        xs[h, :, BLK : 2 * BLK] = xall[h, 3 * c]
        xs[h, :, 2 * BLK : 3 * BLK] = xall[h, 1 + c]
    g1[c, :, BLK : 2 * BLK] = gall[3 * c]
    g1[c, :, 2 * BLK : 3 * BLK] = gall[1 + c]
    gpar1[c] = gall[1 + p]

    loaded("fwd", "back")

    inner_window = lambda h: jnp.concatenate([g1[h, :, own], gpar1[h]], axis=1)
    filter_norm(0, inner_window, slice(0, BLK), inner, (c,))
    from_partner(GV, gv.at[p])
    spread_groups(p)

    @pl.when(head)
    def _():
        forth.wait_recv()
        gate(0, outside, gnear, halves=(c,))
        back_again.start()

    loaded("wo1")
    share(wo, WO, 1)

    from_partner(RESP, resp.at[0, p])
    from_partner(WO, wo.at[0, p])
    from_partner(GINN, g1.at[p, :, inn])
    from_partner(PAR1, gpar1.at[p])
    from_partner(GMID, g1.at[p, :, mid])
    filter_norm(0, inner_window, slice(0, BLK), inner, (p,))
    advance(0, inner)
    gate(1, inner, g2, arrived=lambda: from_partner(WVG + 1, wvg.at[1, p]))
    to_partner(PAR2, g2.at[:, :, inn], gpar2)
    pl.when(later)(lambda: respond(1))
    share(resp, RESP, 1, later)

    @pl.when(early)
    def _():
        from_partner(BACK, g1.at[(p, *near)])
        forth.wait_send()

    @pl.when(jnp.logical_and(has_outer, past))
    def _():
        from_outer(NEAR, lambda core: xs.at[(core, *near)])
        gate(0, outside, g1, arrived=lambda: from_partner(WVG, wvg.at[0, p]))

    @pl.when(jnp.logical_not(has_outer))
    def _():
        pl.when(past)(lambda: from_partner(WVG, wvg.at[0, p]))
        xs[:, :, outside] = jnp.zeros((2, xs.shape[1], BLK), BF16)
        g1[:, :, outside] = jnp.zeros_like(gfar)
        gfar[...] = jnp.zeros_like(gfar)

    @pl.when(has_outer)
    def _():
        from_outer(FAR, lambda core: gfar.at[core])

    filter_norm(0, lambda h: jnp.concatenate([gfar[h], g1[h]], axis=1), slice(0, 2 * BLK), outward)
    advance(0, outward)
    exists = jnp.where(has_outer, 1.0, 0.0)
    gate(1, outward, g2, jnp.concatenate([jnp.full((1, BLK), exists, F32), jnp.ones((1, BLK), F32)], axis=1))
    from_partner(PAR2, gpar2)
    from_partner(RESP + 1, resp.at[1, p])
    from_partner(WO + 1, wo.at[1, p])
    filter_norm(1, lambda h: jnp.concatenate([g2[h], gpar2[h]], axis=1), slice(0, 2 * BLK), own)

    columns = lambda core: (
        pl.ds(pl.multiple_of(core * 3 * BLK, BLK), BLK),
        pl.ds(pl.multiple_of((1 + core) * BLK, BLK), BLK),
    )
    whole = slice(0, 2 * BLK)
    project_out(1, p, own, obuf.at[0], whole)
    for q in range(2):
        part = pl.ds(2 * q * BLK, 2 * BLK)
        for k, lane in enumerate(columns(c)):
            to_partner(OMID + 2 * q + k, obuf.at[0, part, pl.ds(k * BLK, BLK)], o_ref.at[part, lane])
    project_out(1, c, own, obuf.at[1], whole)
    for k, lane in enumerate(columns(c)):
        o_ref[:, lane] = obuf[1, :, k * BLK : (k + 1) * BLK]
    for copies in (near_copies, far_copies):
        for there, copy in zip((has_left, has_right), copies):
            pl.when(there)(copy.wait_send)
    for when, copy in sent:
        if when is None:
            copy.wait_send()
        else:
            pl.when(when)(copy.wait_send)
    pl.when(head)(back_again.wait_send)
    for q in range(2):
        part = pl.ds(2 * q * BLK, 2 * BLK)
        for k, lane in enumerate(columns(p)):
            from_partner(OMID + 2 * q + k, o_ref.at[part, lane])


def scoped(n_sp, *refs):
    pl.run_scoped(
        lambda *semaphores: kernel(n_sp, *refs, *semaphores),
        pltpu.SemaphoreType.DMA((11,)),
        pltpu.SemaphoreType.DMA((22,)),
    )


def write_kernel(src, dst, sem):
    copy = pltpu.make_async_copy(src, dst, sem)
    copy.start()
    copy.wait()


def write_out(value):
    return pl.pallas_call(
        write_kernel,
        out_shape=jax.ShapeDtypeStruct(value.shape, value.dtype),
        in_specs=[pl.BlockSpec(memory_space=pltpu.VMEM)],
        out_specs=pl.BlockSpec(memory_space=pl.ANY),
        scratch_shapes=[pltpu.SemaphoreType.DMA],
        compiler_params=pltpu.CompilerParams(vmem_limit_bytes=1024 * 1024),
    )(pltpu.with_memory_space_constraint(value, pltpu.VMEM))


def solution(mesh):
    n_sp = mesh.shape["sp"]

    def body(stream, norm_gain, w_value, w_gate, conv_taps, group_gain, group_shift, w_out):
        layers, features = norm_gain.shape
        half_features, tokens = stream.shape
        channels = w_value.shape[1]
        taps = conv_taps.shape[2]
        any_spec = pl.BlockSpec(memory_space=pl.ANY)
        vmem = pltpu.VMEM
        result = pl.pallas_call(
            functools.partial(scoped, n_sp),
            out_shape=pltpu.VMEM(stream.shape, stream.dtype),
            in_specs=[any_spec] * 11,
            out_specs=pl.BlockSpec(memory_space=pltpu.VMEM),
            scratch_shapes=[
                vmem((2, 4, half_features, BLK), BF16),
                vmem((2, half_features, 3 * BLK), BF16),
                vmem((layers, 2, 2, BLK, features), BF16),
                vmem((layers, 2, 2, 2, BLK, features), BF16),
                vmem((layers, 2, half_features, 2 * channels), BF16),
                vmem((2 * BLK, layers, channels), BF16),
                vmem((layers, features), F32),
                vmem((2, 2, layers, channels), F32),
                vmem((layers, 2, channels, BLK), F32),
                vmem((layers, 2, channels, BLK), F32),
                vmem((layers, 2, channels, SIZE), BF16),
                vmem((SIZE, SIZE), BF16),
                vmem((SIZE, 2 * BLK), BF16),
                vmem((layers, SIZE, SIZE), BF16),
                vmem((2, 2 * BLK, tokens), F32),
                vmem((4, channels, BLK), BF16),
                vmem((2, channels, 3 * BLK), BF16),
                vmem((2, channels, 3 * BLK), BF16),
                vmem((2, channels, BLK), BF16),
                vmem((2, channels, BLK), BF16),
                vmem((2, channels, BLK), BF16),
                vmem((2, channels, BLK), BF16),
                vmem((2, channels, 3 * BLK), BF16),
                vmem((2, half_features, 2 * BLK), BF16),
                pltpu.SemaphoreType.DMA((22,)),
                pltpu.SemaphoreType.REGULAR,
            ],
            compiler_params=pltpu.CompilerParams(
                collective_id=0, has_side_effects=True, vmem_limit_bytes=60 * 1024 * 1024
            ),
        )(
            stream, norm_gain, w_value, w_gate, jnp.transpose(conv_taps, (2, 0, 1)),
            group_gain, group_shift, w_out, *tables(taps),
        )
        return write_out(result)

    placed = (
        P("tp", "sp"),
        P(),
        P(None, "tp", None),
        P(None, "tp", None),
        P(None, "tp", None),
        P(None, "tp"),
        P(None, "tp"),
        P(None, "tp", None),
    )
    return jax.shard_map(body, mesh=mesh, in_specs=placed, out_specs=P("tp", "sp"), check_vma=False)
```

```python
import functools

import jax
import jax.numpy as jnp
import numpy as np
from jax import lax
from jax.experimental import pallas as pl
from jax.experimental.pallas import tpu as pltpu
from jax.sharding import PartitionSpec as P

MESH = pl.DeviceIdType.MESH
BLK = 128
SIZE = 512
HALF = SIZE // 2
RMS_EPS = 1e-06
LN_EPS = 1e-05
F32 = jnp.float32
BF16 = jnp.bfloat16


def tables(taps):
    angle = lambda t: np.asarray(t)[:, None] * ((np.arange(HALF) + 0.5) * (2 * np.pi / SIZE))[None]
    trig = lambda t: np.stack([np.cos(angle(t)), np.sin(angle(t))], axis=1).reshape(
        -1, 2, 2, BLK
    ).transpose(0, 2, 1, 3).reshape(-1, SIZE)
    blocks = [np.arange(BLK) + BLK * b for b in range(4)]
    reach = (taps - 1) // 2
    forward = [np.concatenate([trig(blocks[b]) for b in order]) for order in ((0, 1, 2, 3), (3, 2, 1, 0))]
    back = [
        np.concatenate([trig(blocks[b] - reach).T for b in order], axis=1) * (2.0 / SIZE)
        for order in ((1, 2), (2, 1))
    ]
    mixed = np.zeros((2, 2 * BLK, 2, 2 * HALF))
    for layer in range(2):
        mixed[layer, :taps, layer] = trig(np.arange(taps))
    return (
        jnp.asarray(np.stack(forward), BF16),
        jnp.asarray(np.stack(back), BF16),
        jnp.asarray(mixed.reshape(2, 4 * BLK, SIZE), BF16),
    )


def kernel(
    n_sp,
    x_hbm, ng_hbm, wv_hbm, wg_hbm, taps_hbm, gg_hbm, gs_hbm, wo_hbm, fwd_hbm, back_hbm, ftap_hbm,
    o_ref,
    xall, xs, wraw, wvg, wo, taps, ngv, gv, ggb, gsb, resp, fwd, back, ftap,
    acc, begun, gall, g1, g2, gfar, gnear, gpar1, gpar2, act, obuf,
    rsem, ready, lsem, ssem,
):
    sp, c = lax.axis_index("sp"), lax.axis_index("tp")
    p = 1 - c
    outer = sp + 2 * c - 1
    has_left = sp > 0
    has_right = sp < n_sp - 1
    has_outer = jnp.logical_and(outer >= 0, outer < n_sp)
    first = sp == 0
    head = jnp.logical_and(first, c == 0)
    early = jnp.logical_and(first, c == 1)
    later = jnp.logical_not(early)
    past = sp > 0
    left_count = jnp.where(has_left, 1, 0)
    right_count = jnp.where(has_right, 1, 0)
    layers, features = ng_hbm.shape

    local = {}

    def load(name, pairs, whole):
        sem = lsem.at[len(local)]
        for src, dst in pairs:
            pltpu.make_async_copy(src, dst, sem).start()
        local[name] = pltpu.make_async_copy(whole, whole, sem)

    def loaded(*names):
        for name in names:
            local[name].wait()

    def load_wvg(l):
        pairs = []
        for k in range(2):
            pairs.append((wv_hbm.at[l, pl.ds(k * BLK, BLK)], wraw.at[l, k, 0]))
            pairs.append((wg_hbm.at[l, pl.ds(k * BLK, BLK)], wraw.at[l, k, 1]))
        load(f"w{l}", pairs, wraw.at[l])

    load("x", [(x_hbm, xall.at[c])], xall.at[c])

    barrier = pltpu.get_barrier_semaphore()
    pl.semaphore_signal(barrier, inc=1, device_id=(sp, p), device_id_type=MESH)

    @pl.when(has_outer)
    def _():
        pl.semaphore_signal(barrier, inc=1, device_id=(outer, 1), device_id_type=MESH)

    load("ng", [(ng_hbm, ngv)], ngv)
    load("groups", [(gg_hbm, gv.at[c, 0]), (gs_hbm, gv.at[c, 1])], gv.at[c])
    load_wvg(0)
    load("wo0", [(wo_hbm.at[0], wo.at[0, c])], wo.at[0, c])
    tap_rows = taps.at[pl.ds(0, taps_hbm.shape[0])]
    load("taps", [(taps_hbm, tap_rows)], tap_rows)
    load("ftap", [(ftap_hbm, ftap)], ftap)
    load_wvg(1)
    load("fwd", [(fwd_hbm.at[c], fwd)], fwd)
    load("back", [(back_hbm.at[c], back)], back)
    load("wo1", [(wo_hbm.at[1], wo.at[1, c])], wo.at[1, c])

    NEAR, FAR, X, GMID, GINN, WVG, WO, RESP, GV, PAR1, PAR2, OMID = 0, 2, 4, 5, 6, 7, 9, 11, 13, 14, 15, 16
    FORTH, BACK = 20, 21
    sent = []

    def remote(k, src, dst, device):
        return pltpu.make_async_remote_copy(
            src_ref=src, dst_ref=dst, send_sem=ssem.at[k], recv_sem=rsem.at[k],
            device_id=device, device_id_type=MESH,
        )

    def to_partner(k, src, dst, when=None):
        copy = remote(k, src, dst, (sp, p))
        if when is None:
            copy.start()
        else:
            pl.when(when)(copy.start)
        if when is not later:
            sent.append((None if when is early else when, copy))

    def share(ref, k, l, when=None):
        to_partner(k + l, ref.at[l, c], ref.at[l, c], when)

    def from_partner(k, dst):
        remote(k, dst, dst, (sp, p)).wait_recv()

    def to_neighbour(first, direction, src, dst):
        return pltpu.make_async_remote_copy(
            src_ref=src, dst_ref=dst, send_sem=ssem.at[first + direction], recv_sem=rsem.at[first + c],
            device_id=(sp + 2 * direction - 1, 1 - direction), device_id_type=MESH,
        )

    def from_outer(first, part):
        for core in range(2):
            dst = part(core)
            pltpu.make_async_remote_copy(
                src_ref=dst, dst_ref=dst, send_sem=ssem.at[first], recv_sem=rsem.at[first + core],
                device_id=(outer, core), device_id_type=MESH,
            ).wait_recv()

    def start_both(copies):
        for there, copy in zip((has_left, has_right), copies):
            pl.when(there)(copy.start)

    def scale_weights(l):
        gain = ngv[l : l + 1]
        for k in range(2):
            for half in range(2):
                wvg[l, c, k, half] = (wraw[l, k, half].astype(F32) * gain).astype(BF16)

    def spread_groups(h):
        column = lambda row: jnp.broadcast_to(row * 0.5, (BLK, BLK)).T
        for l in range(layers):
            for b in range(2):
                lanes = slice(b * BLK, (b + 1) * BLK)
                ggb[l, h, lanes] = column(gv[h, 0, l : l + 1, lanes])
                gsb[l, h, lanes] = column(gv[h, 1, l : l + 1, lanes])

    def prepare_gates():
        loaded("groups")
        spread_groups(c)
        loaded("ng", "w0")
        scale_weights(0)

    def prepare_taps():
        loaded("taps", "ftap")
        taps[taps_hbm.shape[0] :] = jnp.zeros((taps.shape[0] - taps_hbm.shape[0], *taps.shape[1:]), BF16)

    def respond(l):
        rows = taps[...].reshape(layers * taps.shape[0], taps.shape[2])
        resp[l, c] = lax.dot_general(
            rows, ftap[l], (((0,), (0,)), ((), ())), preferred_element_type=F32
        ).astype(BF16)

    def prepare_weights():
        loaded("w1")
        scale_weights(1)

    @pl.when(early)
    def _():
        prepare_gates()
        prepare_taps()
        for l in range(layers):
            respond(l)
        prepare_weights()

    @pl.when(c == 0)
    def _():
        pl.semaphore_wait(barrier, 1)
        pl.semaphore_signal(ready, inc=1, device_id=(sp, 1), device_id_type=MESH)

    @pl.when(c == 1)
    def _():
        pl.semaphore_wait(ready, 1)

    loaded("x")
    to_partner(X, xall.at[c], xall.at[c])

    @pl.when(c == 1)
    def _():
        pl.semaphore_wait(barrier, 1 + left_count + right_count)
        pl.semaphore_signal(ready, inc=1, device_id=(sp, 0), device_id_type=MESH)

    @pl.when(c == 0)
    def _():
        pl.semaphore_wait(ready, 1)

    near = (slice(None), pl.ds(0, BLK))
    near_copies = [to_neighbour(NEAR, d, xall.at[c, :, pl.ds(3 * d * BLK, BLK)], xs.at[(c, *near)]) for d in range(2)]
    start_both(near_copies)

    pl.when(later)(prepare_gates)
    to_partner(GV, gv.at[c], gv.at[c])
    loaded("wo0")
    share(wo, WO, 0)
    for l in range(layers):
        share(resp, RESP, l, early)

    def squares(x):
        wide = x.astype(F32)
        return jnp.sum(wide * wide, axis=0, keepdims=True)

    def half_inverse(total):
        return 0.5 * lax.rsqrt(total * (1.0 / features) + RMS_EPS)

    def gated(r, inverse, kept):
        value = r[:BLK] * kept
        return (value * jnp.tanh(r[BLK:] * inverse) + value).astype(BF16)

    def gate(l, lanes, dst, exists=None, arrived=None, halves=(0, 1)):
        x = xs[:, :, lanes].reshape(features, lanes.stop - lanes.start)
        inverse = half_inverse(squares(x))
        kept = inverse if exists is None else inverse * exists
        for h in halves if arrived is None else (c, p):
            if h is p:
                arrived()
            for k in range(2):
                r = jnp.dot(wvg[l, h, k].reshape(2 * BLK, features), x, preferred_element_type=F32)
                dst[h, k * BLK : (k + 1) * BLK, lanes] = gated(r, inverse, kept)

    def begin_filter(ready):
        for h in range(2):
            for q in range(2):
                both = slice(2 * q * BLK, 2 * (q + 1) * BLK)
                begun[h, :, both] = jnp.dot(ready(h), fwd[2 * BLK :, both], preferred_element_type=F32)

    def filter_norm(l, window, outputs, lanes, halves=(0, 1), is_begun=False):
        n = outputs.stop - outputs.start
        for h in halves:
            w = window(h)
            filtered = None
            for q in range(2):
                both, re, im = (slice(2 * q * BLK + i * BLK, 2 * q * BLK + j * BLK) for i, j in ((0, 2), (0, 1), (1, 2)))
                g = jnp.dot(w, fwd[: w.shape[1], both], preferred_element_type=F32)
                if is_begun:
                    g = g + begun[h, :, both]
                gr, gi = g[:, :BLK], g[:, BLK:]
                hr, hi = resp[l, h, :, re].astype(F32), resp[l, h, :, im].astype(F32)
                y = jnp.concatenate([(gr * hr + gi * hi).astype(BF16), (gi * hr - gr * hi).astype(BF16)], axis=1)
                term = jnp.dot(y, back[both, outputs], preferred_element_type=F32)
                filtered = term if filtered is None else filtered + term
            for k in range(2):
                part = slice(k * BLK, (k + 1) * BLK)
                f = filtered[part]
                centred = f - jnp.sum(f, axis=0, keepdims=True) * (1.0 / BLK)
                variance = jnp.sum(centred * centred, axis=0, keepdims=True) * (1.0 / BLK)
                gain, shift = ggb[l, h, part], gsb[l, h, part]
                if n > BLK:
                    gain = jnp.concatenate([gain] * (n // BLK), axis=1)
                    shift = jnp.concatenate([shift] * (n // BLK), axis=1)
                s = centred * lax.rsqrt(variance + LN_EPS) * gain + shift
                act[h, part, lanes] = (s * jnp.tanh(s) + s).astype(BF16)

    def project_out(l, h, lanes, dst, dst_lanes, pieces=((0, 2 * BLK), (2 * BLK, 2 * BLK))):
        for first, size in pieces:
            part = slice(first, first + size)
            branch = None
            for g in range(2):
                group = slice(g * 2 * BLK, (g + 1) * 2 * BLK)
                term = jnp.dot(wo[l, h, part, group], act[g, :, lanes], preferred_element_type=F32)
                branch = term if branch is None else branch + term
            dst[part, dst_lanes] = (xs[h, part, lanes].astype(F32) + branch).astype(BF16)

    def advance(l, lanes):
        for h in range(2):
            project_out(l, h, lanes, xs.at[h], lanes)

    columns = lambda core: (
        pl.ds(pl.multiple_of(core * 3 * BLK, BLK), BLK),
        pl.ds(pl.multiple_of((1 + core) * BLK, BLK), BLK),
    )
    own, outside = slice(BLK, 3 * BLK), slice(0, BLK)
    inner, outward = slice(2 * BLK, 3 * BLK), slice(0, 2 * BLK)

    part_rows = features // 2

    def part_dot(core, k):
        x = xall[core]
        w = wvg[0, c, k, :, :, pl.ds(pl.multiple_of(core * part_rows, part_rows), part_rows)]
        return jnp.dot(w.reshape(2 * BLK, part_rows), x, preferred_element_type=F32)

    def part_squares(core):
        return squares(xall[core])

    for k in range(2):
        acc[k] = part_dot(c, k)
    total = part_squares(c)
    near_block = xs.at[(slice(None), *near)]
    forth = remote(FORTH, near_block, near_block, (sp, p))
    back_again = remote(BACK, gnear.at[c], g1.at[(c, *near)], (sp, p))

    @pl.when(early)
    def _():
        from_outer(NEAR, lambda core: xs.at[(core, *near)])
        forth.start()
        gate(0, outside, g1, halves=(c,))

    from_partner(X, xall.at[p])
    inverse = half_inverse(total + part_squares(p))
    for k in range(2):
        gk = gated(acc[k] + part_dot(p, k), inverse, inverse)
        for b in range(4):
            gall[b, k * BLK : (k + 1) * BLK] = gk[:, b * BLK : (b + 1) * BLK]
    mid, inn = pl.ds(BLK, BLK), pl.ds(2 * BLK, BLK)
    to_partner(GINN, gall.at[1 + p], g1.at[c, :, inn])
    to_partner(PAR1, gall.at[1 + c], gpar1.at[c])
    to_partner(GMID, gall.at[3 * p], g1.at[c, :, mid])
    far_copies = [to_neighbour(FAR, d, gall.at[1 + d], gfar.at[c]) for d in range(2)]
    start_both(far_copies)

    @pl.when(later)
    def _():
        prepare_taps()
        respond(0)

    share(resp, RESP, 0, later)
    pl.when(later)(prepare_weights)
    share(wvg, WVG, 1)
    share(wvg, WVG, 0, past)
    for h in range(2):
        for place, lane in zip((1, 2), columns(c)):
            xs[h, :, place * BLK : (place + 1) * BLK] = xall[h, :, lane]
    g1[c, :, BLK : 2 * BLK] = gall[3 * c]
    g1[c, :, 2 * BLK : 3 * BLK] = gall[1 + c]
    gpar1[c] = gall[1 + p]

    loaded("fwd", "back")

    inner_window = lambda h: jnp.concatenate([g1[h, :, own], gpar1[h]], axis=1)
    filter_norm(0, inner_window, slice(0, BLK), inner, (c,))
    from_partner(GV, gv.at[p])
    spread_groups(p)

    @pl.when(head)
    def _():
        forth.wait_recv()
        gate(0, outside, gnear, halves=(c,))
        back_again.start()

    loaded("wo1")
    share(wo, WO, 1)

    from_partner(RESP, resp.at[0, p])
    from_partner(WO, wo.at[0, p])
    from_partner(GINN, g1.at[p, :, inn])
    from_partner(PAR1, gpar1.at[p])
    from_partner(GMID, g1.at[p, :, mid])
    filter_norm(0, inner_window, slice(0, BLK), inner, (p,))
    advance(0, inner)
    def layer_1_weights():
        begin_filter(lambda h: g1[h, :, own])
        from_partner(WVG + 1, wvg.at[1, p])

    gate(1, inner, g2, arrived=layer_1_weights)
    to_partner(PAR2, g2.at[:, :, inn], gpar2)
    pl.when(later)(lambda: respond(1))
    share(resp, RESP, 1, later)

    @pl.when(early)
    def _():
        from_partner(BACK, g1.at[(p, *near)])
        forth.wait_send()

    @pl.when(jnp.logical_and(has_outer, past))
    def _():
        from_outer(NEAR, lambda core: xs.at[(core, *near)])
        gate(0, outside, g1, arrived=lambda: from_partner(WVG, wvg.at[0, p]))

    @pl.when(jnp.logical_not(has_outer))
    def _():
        pl.when(past)(lambda: from_partner(WVG, wvg.at[0, p]))
        xs[:, :, outside] = jnp.zeros((2, xs.shape[1], BLK), BF16)
        g1[:, :, outside] = jnp.zeros_like(gfar)
        gfar[...] = jnp.zeros_like(gfar)

    @pl.when(has_outer)
    def _():
        from_outer(FAR, lambda core: gfar.at[core])

    filter_norm(
        0, lambda h: jnp.concatenate([gfar[h], g1[h, :, outside]], axis=1), slice(0, 2 * BLK), outward, is_begun=True
    )
    advance(0, outward)
    exists = jnp.where(has_outer, 1.0, 0.0)
    gate(1, outward, g2, jnp.concatenate([jnp.full((1, BLK), exists, F32), jnp.ones((1, BLK), F32)], axis=1))
    from_partner(PAR2, gpar2)
    from_partner(RESP + 1, resp.at[1, p])
    from_partner(WO + 1, wo.at[1, p])
    filter_norm(1, lambda h: jnp.concatenate([g2[h], gpar2[h]], axis=1), slice(0, 2 * BLK), own)

    whole = slice(0, 2 * BLK)
    project_out(1, p, own, obuf.at[0], whole)
    for q in range(2):
        part = pl.ds(2 * q * BLK, 2 * BLK)
        for k, lane in enumerate(columns(c)):
            to_partner(OMID + 2 * q + k, obuf.at[0, part, pl.ds(k * BLK, BLK)], o_ref.at[part, lane])
    project_out(1, c, own, obuf.at[1], whole)
    for k, lane in enumerate(columns(c)):
        o_ref[:, lane] = obuf[1, :, k * BLK : (k + 1) * BLK]
    for copies in (near_copies, far_copies):
        for there, copy in zip((has_left, has_right), copies):
            pl.when(there)(copy.wait_send)
    for when, copy in sent:
        if when is None:
            copy.wait_send()
        else:
            pl.when(when)(copy.wait_send)
    pl.when(head)(back_again.wait_send)
    for q in range(2):
        part = pl.ds(2 * q * BLK, 2 * BLK)
        for k, lane in enumerate(columns(p)):
            from_partner(OMID + 2 * q + k, o_ref.at[part, lane])


def scoped(n_sp, *refs):
    pl.run_scoped(
        lambda *semaphores: kernel(n_sp, *refs, *semaphores),
        pltpu.SemaphoreType.DMA((11,)),
        pltpu.SemaphoreType.DMA((22,)),
    )


def write_kernel(src, dst, sem):
    copy = pltpu.make_async_copy(src, dst, sem)
    copy.start()
    copy.wait()


def write_out(value):
    return pl.pallas_call(
        write_kernel,
        out_shape=jax.ShapeDtypeStruct(value.shape, value.dtype),
        in_specs=[pl.BlockSpec(memory_space=pltpu.VMEM)],
        out_specs=pl.BlockSpec(memory_space=pl.ANY),
        scratch_shapes=[pltpu.SemaphoreType.DMA],
        compiler_params=pltpu.CompilerParams(vmem_limit_bytes=1024 * 1024),
    )(pltpu.with_memory_space_constraint(value, pltpu.VMEM))


def solution(mesh):
    n_sp = mesh.shape["sp"]

    def body(stream, norm_gain, w_value, w_gate, conv_taps, group_gain, group_shift, w_out):
        layers, features = norm_gain.shape
        half_features, tokens = stream.shape
        channels = w_value.shape[1]
        taps = conv_taps.shape[2]
        any_spec = pl.BlockSpec(memory_space=pl.ANY)
        vmem = pltpu.VMEM
        result = pl.pallas_call(
            functools.partial(scoped, n_sp),
            out_shape=pltpu.VMEM(stream.shape, stream.dtype),
            in_specs=[any_spec] * 11,
            out_specs=pl.BlockSpec(memory_space=pltpu.VMEM),
            scratch_shapes=[
                vmem((2, half_features, tokens), BF16),
                vmem((2, half_features, 3 * BLK), BF16),
                vmem((layers, 2, 2, BLK, features), BF16),
                vmem((layers, 2, 2, 2, BLK, features), BF16),
                vmem((layers, 2, half_features, 2 * channels), BF16),
                vmem((2 * BLK, layers, channels), BF16),
                vmem((layers, features), F32),
                vmem((2, 2, layers, channels), F32),
                vmem((layers, 2, channels, BLK), F32),
                vmem((layers, 2, channels, BLK), F32),
                vmem((layers, 2, channels, SIZE), BF16),
                vmem((SIZE, SIZE), BF16),
                vmem((SIZE, 2 * BLK), BF16),
                vmem((layers, SIZE, SIZE), BF16),
                vmem((2, 2 * BLK, tokens), F32),
                vmem((2, channels, SIZE), F32),
                vmem((4, channels, BLK), BF16),
                vmem((2, channels, 3 * BLK), BF16),
                vmem((2, channels, 3 * BLK), BF16),
                vmem((2, channels, BLK), BF16),
                vmem((2, channels, BLK), BF16),
                vmem((2, channels, BLK), BF16),
                vmem((2, channels, BLK), BF16),
                vmem((2, channels, 3 * BLK), BF16),
                vmem((2, half_features, 2 * BLK), BF16),
                pltpu.SemaphoreType.DMA((22,)),
                pltpu.SemaphoreType.REGULAR,
            ],
            compiler_params=pltpu.CompilerParams(
                collective_id=0, has_side_effects=True, vmem_limit_bytes=60 * 1024 * 1024
            ),
        )(
            stream, norm_gain, w_value, w_gate, jnp.transpose(conv_taps, (2, 0, 1)),
            group_gain, group_shift, w_out, *tables(taps),
        )
        return write_out(result)

    placed = (
        P("tp", "sp"),
        P(),
        P(None, "tp", None),
        P(None, "tp", None),
        P(None, "tp", None),
        P(None, "tp"),
        P(None, "tp"),
        P(None, "tp", None),
    )
    return jax.shard_map(body, mesh=mesh, in_specs=placed, out_specs=P("tp", "sp"), check_vma=False)
```

```python
import functools

import jax
import jax.numpy as jnp
import numpy as np
from jax import lax
from jax.experimental import pallas as pl
from jax.experimental.pallas import tpu as pltpu
from jax.sharding import PartitionSpec as P

MESH = pl.DeviceIdType.MESH
BLK = 128
SIZE = 512
HALF = SIZE // 2
RMS_EPS = 1e-06
LN_EPS = 1e-05
F32 = jnp.float32
BF16 = jnp.bfloat16


def tables(taps):
    angle = lambda t: np.asarray(t)[:, None] * ((np.arange(HALF) + 0.5) * (2 * np.pi / SIZE))[None]
    trig = lambda t: np.stack([np.cos(angle(t)), np.sin(angle(t))], axis=1).reshape(
        -1, 2, 2, BLK
    ).transpose(0, 2, 1, 3).reshape(-1, SIZE)
    blocks = [np.arange(BLK) + BLK * b for b in range(4)]
    reach = (taps - 1) // 2
    forward = [np.concatenate([trig(blocks[b]) for b in order]) for order in ((0, 1, 2, 3), (3, 2, 1, 0))]
    back = [
        np.concatenate([trig(blocks[b] - reach).T for b in order], axis=1) * (2.0 / SIZE)
        for order in ((1, 2), (2, 1))
    ]
    mixed = np.zeros((2, 2 * BLK, 2, 2 * HALF))
    for layer in range(2):
        mixed[layer, :taps, layer] = trig(np.arange(taps))
    return (
        jnp.asarray(np.stack(forward), BF16),
        jnp.asarray(np.stack(back), BF16),
        jnp.asarray(mixed.reshape(2, 4 * BLK, SIZE), BF16),
    )


def kernel(
    n_sp,
    x_hbm, ng_hbm, wv_hbm, wg_hbm, taps_hbm, gg_hbm, gs_hbm, wo_hbm, fwd_hbm, back_hbm, ftap_hbm,
    o_ref,
    xall, xs, wraw, wvg, wo, taps, ngv, gv, ggb, gsb, resp, fwd, back, ftap,
    acc, begun, begun_last, gall, g1, g2, gfar, gnear, gpar1, gpar2, act, obuf,
    rsem, ready, lsem, ssem,
):
    sp, c = lax.axis_index("sp"), lax.axis_index("tp")
    p = 1 - c
    outer = sp + 2 * c - 1
    has_left = sp > 0
    has_right = sp < n_sp - 1
    has_outer = jnp.logical_and(outer >= 0, outer < n_sp)
    first = sp == 0
    head = jnp.logical_and(first, c == 0)
    early = jnp.logical_and(first, c == 1)
    later = jnp.logical_not(early)
    past = sp > 0
    slow = jnp.logical_and(past, lax.rem(sp, 16) == 0)
    prompt = jnp.logical_not(slow)
    left_count = jnp.where(has_left, 1, 0)
    right_count = jnp.where(has_right, 1, 0)
    layers, features = ng_hbm.shape

    local = {}

    def load(name, pairs, whole):
        sem = lsem.at[len(local)]
        for src, dst in pairs:
            pltpu.make_async_copy(src, dst, sem).start()
        local[name] = pltpu.make_async_copy(whole, whole, sem)

    def loaded(*names):
        for name in names:
            local[name].wait()

    def load_wvg(l):
        pairs = []
        for k in range(2):
            pairs.append((wv_hbm.at[l, pl.ds(k * BLK, BLK)], wraw.at[l, k, 0]))
            pairs.append((wg_hbm.at[l, pl.ds(k * BLK, BLK)], wraw.at[l, k, 1]))
        load(f"w{l}", pairs, wraw.at[l])

    load("x", [(x_hbm, xall.at[c])], xall.at[c])

    barrier = pltpu.get_barrier_semaphore()
    pl.semaphore_signal(barrier, inc=1, device_id=(sp, p), device_id_type=MESH)

    @pl.when(has_outer)
    def _():
        pl.semaphore_signal(barrier, inc=1, device_id=(outer, 1), device_id_type=MESH)

    load("ng", [(ng_hbm, ngv)], ngv)
    load("groups", [(gg_hbm, gv.at[c, 0]), (gs_hbm, gv.at[c, 1])], gv.at[c])
    load_wvg(0)
    load("wo0", [(wo_hbm.at[0], wo.at[0, c])], wo.at[0, c])
    tap_rows = taps.at[pl.ds(0, taps_hbm.shape[0])]
    load("taps", [(taps_hbm, tap_rows)], tap_rows)
    load("ftap", [(ftap_hbm, ftap)], ftap)
    load_wvg(1)
    load("fwd", [(fwd_hbm.at[c], fwd)], fwd)
    load("back", [(back_hbm.at[c], back)], back)
    load("wo1", [(wo_hbm.at[1], wo.at[1, c])], wo.at[1, c])

    NEAR, FAR, X, GMID, GINN, WVG, WO, RESP, GV, PAR1, PAR2, OMID = 0, 2, 4, 5, 6, 7, 9, 11, 13, 14, 15, 16
    FORTH, BACK = 20, 21
    sent = []

    def remote(k, src, dst, device):
        return pltpu.make_async_remote_copy(
            src_ref=src, dst_ref=dst, send_sem=ssem.at[k], recv_sem=rsem.at[k],
            device_id=device, device_id_type=MESH,
        )

    def to_partner(k, src, dst, when=None):
        copy = remote(k, src, dst, (sp, p))
        if when is None:
            copy.start()
        else:
            pl.when(when)(copy.start)
        if when is not later:
            sent.append((None if when is early else when, copy))

    def share(ref, k, l, when=None):
        to_partner(k + l, ref.at[l, c], ref.at[l, c], when)

    def from_partner(k, dst):
        remote(k, dst, dst, (sp, p)).wait_recv()

    def to_neighbour(first, direction, src, dst):
        return pltpu.make_async_remote_copy(
            src_ref=src, dst_ref=dst, send_sem=ssem.at[first + direction], recv_sem=rsem.at[first + c],
            device_id=(sp + 2 * direction - 1, 1 - direction), device_id_type=MESH,
        )

    def from_outer(first, part):
        for core in range(2):
            dst = part(core)
            pltpu.make_async_remote_copy(
                src_ref=dst, dst_ref=dst, send_sem=ssem.at[first], recv_sem=rsem.at[first + core],
                device_id=(outer, core), device_id_type=MESH,
            ).wait_recv()

    def start_both(copies):
        for there, copy in zip((has_left, has_right), copies):
            pl.when(there)(copy.start)

    def scale_weights(l):
        gain = ngv[l : l + 1]
        for k in range(2):
            for half in range(2):
                wvg[l, c, k, half] = (wraw[l, k, half].astype(F32) * gain).astype(BF16)

    def spread_groups(h):
        column = lambda row: jnp.broadcast_to(row * 0.5, (BLK, BLK)).T
        for l in range(layers):
            for b in range(2):
                lanes = slice(b * BLK, (b + 1) * BLK)
                ggb[l, h, lanes] = column(gv[h, 0, l : l + 1, lanes])
                gsb[l, h, lanes] = column(gv[h, 1, l : l + 1, lanes])

    def prepare_gates():
        loaded("groups")
        spread_groups(c)
        loaded("ng", "w0")
        scale_weights(0)

    def prepare_taps():
        loaded("taps", "ftap")
        taps[taps_hbm.shape[0] :] = jnp.zeros((taps.shape[0] - taps_hbm.shape[0], *taps.shape[1:]), BF16)

    def respond(l):
        rows = taps[...].reshape(layers * taps.shape[0], taps.shape[2])
        resp[l, c] = lax.dot_general(
            rows, ftap[l], (((0,), (0,)), ((), ())), preferred_element_type=F32
        ).astype(BF16)

    def prepare_weights():
        loaded("w1")
        scale_weights(1)

    @pl.when(early)
    def _():
        prepare_gates()
        prepare_taps()
        for l in range(layers):
            respond(l)
        prepare_weights()

    @pl.when(c == 0)
    def _():
        pl.semaphore_wait(barrier, 1)
        pl.semaphore_signal(ready, inc=1, device_id=(sp, 1), device_id_type=MESH)

    @pl.when(c == 1)
    def _():
        pl.semaphore_wait(ready, 1)

    loaded("x")
    to_partner(X, xall.at[c], xall.at[c])
    wo_copy = remote(WO, wo.at[0, c], wo.at[0, c], (sp, p))
    wvg_copy = remote(WVG, wvg.at[0, c], wvg.at[0, c], (sp, p))
    sent.extend([(None, wo_copy), (past, wvg_copy)])

    @pl.when(slow)
    def _():
        loaded("wo0")
        wo_copy.start()
        prepare_gates()
        wvg_copy.start()

    @pl.when(c == 1)
    def _():
        pl.semaphore_wait(barrier, 1 + left_count + right_count)
        pl.semaphore_signal(ready, inc=1, device_id=(sp, 0), device_id_type=MESH)

    @pl.when(c == 0)
    def _():
        pl.semaphore_wait(ready, 1)

    near = (slice(None), pl.ds(0, BLK))
    near_copies = [to_neighbour(NEAR, d, xall.at[c, :, pl.ds(3 * d * BLK, BLK)], xs.at[(c, *near)]) for d in range(2)]
    start_both(near_copies)

    pl.when(jnp.logical_and(later, prompt))(prepare_gates)
    to_partner(GV, gv.at[c], gv.at[c])

    @pl.when(prompt)
    def _():
        loaded("wo0")
        wo_copy.start()

    for l in range(layers):
        share(resp, RESP, l, early)

    def squares(x):
        wide = x.astype(F32)
        return jnp.sum(wide * wide, axis=0, keepdims=True)

    def half_inverse(total):
        return 0.5 * lax.rsqrt(total * (1.0 / features) + RMS_EPS)

    def gated(r, inverse):
        value = r[:BLK] * inverse
        return (value * jnp.tanh(r[BLK:] * inverse) + value).astype(BF16)

    def gate(l, lanes, dst, arrived=None, halves=(0, 1)):
        x = xs[:, :, lanes].reshape(features, lanes.stop - lanes.start)
        inverse = half_inverse(squares(x))
        for h in halves if arrived is None else (c, p):
            if h is p:
                arrived()
            for k in range(2):
                r = jnp.dot(wvg[l, h, k].reshape(2 * BLK, features), x, preferred_element_type=F32)
                dst[h, k * BLK : (k + 1) * BLK, lanes] = gated(r, inverse)

    def begin_filter(begun, ready):
        for h in range(2):
            for q in range(2):
                both = slice(2 * q * BLK, 2 * (q + 1) * BLK)
                begun[h, :, both] = jnp.dot(ready(h), fwd[2 * BLK :, both], preferred_element_type=F32)

    def filter_norm(l, window, outputs, lanes, halves=(0, 1), begun=None):
        n = outputs.stop - outputs.start
        for h in halves:
            w = window(h)
            filtered = None
            for q in range(2):
                both, re, im = (slice(2 * q * BLK + i * BLK, 2 * q * BLK + j * BLK) for i, j in ((0, 2), (0, 1), (1, 2)))
                g = jnp.dot(w, fwd[: w.shape[1], both], preferred_element_type=F32)
                if begun is not None:
                    g = g + begun[h, :, both]
                gr, gi = g[:, :BLK], g[:, BLK:]
                hr, hi = resp[l, h, :, re].astype(F32), resp[l, h, :, im].astype(F32)
                y = jnp.concatenate([(gr * hr + gi * hi).astype(BF16), (gi * hr - gr * hi).astype(BF16)], axis=1)
                term = jnp.dot(y, back[both, outputs], preferred_element_type=F32)
                filtered = term if filtered is None else filtered + term
            for k in range(2):
                part = slice(k * BLK, (k + 1) * BLK)
                f = filtered[part]
                centred = f - jnp.sum(f, axis=0, keepdims=True) * (1.0 / BLK)
                variance = jnp.sum(centred * centred, axis=0, keepdims=True) * (1.0 / BLK)
                gain, shift = ggb[l, h, part], gsb[l, h, part]
                if n > BLK:
                    gain = jnp.concatenate([gain] * (n // BLK), axis=1)
                    shift = jnp.concatenate([shift] * (n // BLK), axis=1)
                s = centred * lax.rsqrt(variance + LN_EPS) * gain + shift
                act[h, part, lanes] = (s * jnp.tanh(s) + s).astype(BF16)

    def project_out(l, h, lanes, dst, dst_lanes, pieces=((0, 2 * BLK), (2 * BLK, 2 * BLK))):
        for first, size in pieces:
            part = slice(first, first + size)
            branch = None
            for g in range(2):
                group = slice(g * 2 * BLK, (g + 1) * 2 * BLK)
                term = jnp.dot(wo[l, h, part, group], act[g, :, lanes], preferred_element_type=F32)
                branch = term if branch is None else branch + term
            dst[part, dst_lanes] = (xs[h, part, lanes].astype(F32) + branch).astype(BF16)

    def advance(l, lanes):
        for h in range(2):
            project_out(l, h, lanes, xs.at[h], lanes)

    columns = lambda core: (
        pl.ds(pl.multiple_of(core * 3 * BLK, BLK), BLK),
        pl.ds(pl.multiple_of((1 + core) * BLK, BLK), BLK),
    )
    own, outside = slice(BLK, 3 * BLK), slice(0, BLK)
    inner, outward = slice(2 * BLK, 3 * BLK), slice(0, 2 * BLK)

    part_rows = features // 2

    def part_dot(core, k):
        x = xall[core]
        w = wvg[0, c, k, :, :, pl.ds(pl.multiple_of(core * part_rows, part_rows), part_rows)]
        return jnp.dot(w.reshape(2 * BLK, part_rows), x, preferred_element_type=F32)

    def part_squares(core):
        return squares(xall[core])

    for k in range(2):
        acc[k] = part_dot(c, k)
    total = part_squares(c)
    near_block = xs.at[(slice(None), *near)]
    forth = remote(FORTH, near_block, near_block, (sp, p))
    back_again = remote(BACK, gnear.at[c], g1.at[(c, *near)], (sp, p))

    @pl.when(early)
    def _():
        from_outer(NEAR, lambda core: xs.at[(core, *near)])
        forth.start()
        gate(0, outside, g1, halves=(c,))

    from_partner(X, xall.at[p])
    inverse = half_inverse(total + part_squares(p))
    for k in range(2):
        gk = gated(acc[k] + part_dot(p, k), inverse)
        for b in range(4):
            gall[b, k * BLK : (k + 1) * BLK] = gk[:, b * BLK : (b + 1) * BLK]
    mid, inn = pl.ds(BLK, BLK), pl.ds(2 * BLK, BLK)
    to_partner(GINN, gall.at[1 + p], g1.at[c, :, inn])
    to_partner(PAR1, gall.at[1 + c], gpar1.at[c])
    to_partner(GMID, gall.at[3 * p], g1.at[c, :, mid])
    far_copies = [to_neighbour(FAR, d, gall.at[1 + d], gfar.at[c]) for d in range(2)]
    start_both(far_copies)

    @pl.when(later)
    def _():
        prepare_taps()
        respond(0)

    share(resp, RESP, 0, later)
    pl.when(later)(prepare_weights)
    share(wvg, WVG, 1)
    pl.when(jnp.logical_and(past, prompt))(wvg_copy.start)
    for h in range(2):
        for place, lane in zip((1, 2), columns(c)):
            xs[h, :, place * BLK : (place + 1) * BLK] = xall[h, :, lane]
    g1[c, :, BLK : 2 * BLK] = gall[3 * c]
    g1[c, :, 2 * BLK : 3 * BLK] = gall[1 + c]
    gpar1[c] = gall[1 + p]

    loaded("fwd", "back")

    inner_window = lambda h: jnp.concatenate([g1[h, :, own], gpar1[h]], axis=1)
    alone = jnp.logical_not(has_outer)
    inside = jnp.logical_and(has_outer, past)

    @pl.when(has_outer)
    def _():
        filter_norm(0, inner_window, slice(0, BLK), inner, (c,))

    from_partner(GV, gv.at[p])
    spread_groups(p)

    @pl.when(head)
    def _():
        forth.wait_recv()
        gate(0, outside, gnear, halves=(c,))
        back_again.start()

    from_partner(RESP, resp.at[0, p])
    from_partner(WO, wo.at[0, p])
    from_partner(GINN, g1.at[p, :, inn])
    from_partner(PAR1, gpar1.at[p])
    from_partner(GMID, g1.at[p, :, mid])

    @pl.when(has_outer)
    def _():
        def layer_1_weights():
            begin_filter(begun, lambda h: g1[h, :, own])
            from_partner(WVG + 1, wvg.at[1, p])

        filter_norm(0, inner_window, slice(0, BLK), inner, (p,))
        advance(0, inner)
        gate(1, inner, g2, arrived=layer_1_weights)

    @pl.when(alone)
    def _():
        pl.when(past)(lambda: from_partner(WVG, wvg.at[0, p]))
        g1[:, :, outside] = jnp.zeros_like(gfar)
        filter_norm(0, lambda h: jnp.concatenate([g1[h], gpar1[h]], axis=1), slice(0, 2 * BLK), own)
        advance(0, own)
        from_partner(WVG + 1, wvg.at[1, p])
        gate(1, own, g2)
        g2[:, :, outside] = jnp.zeros_like(gfar)

    to_partner(PAR2, g2.at[:, :, inn], gpar2)
    pl.when(later)(lambda: respond(1))
    share(resp, RESP, 1, later)
    loaded("wo1")
    share(wo, WO, 1)

    def begin_last():
        from_partner(PAR2, gpar2)
        begin_filter(begun_last, lambda h: jnp.concatenate([g2[h, :, inner], gpar2[h]], axis=1))

    @pl.when(early)
    def _():
        from_partner(BACK, g1.at[(p, *near)])
        forth.wait_send()

    @pl.when(inside)
    def _():
        from_outer(NEAR, lambda core: xs.at[(core, *near)])
        gate(0, outside, g1, arrived=lambda: from_partner(WVG, wvg.at[0, p]))
        begin_last()

    @pl.when(has_outer)
    def _():
        from_outer(FAR, lambda core: gfar.at[core])
        late = lambda h: jnp.concatenate([gfar[h], g1[h, :, outside]], axis=1)
        filter_norm(0, late, slice(0, 2 * BLK), outward, begun=begun)
        advance(0, outward)
        gate(1, outward, g2)

    pl.when(jnp.logical_not(inside))(begin_last)
    from_partner(RESP + 1, resp.at[1, p])
    filter_norm(1, lambda h: g2[h, :, outward], slice(0, 2 * BLK), own, begun=begun_last)
    from_partner(WO + 1, wo.at[1, p])

    whole = slice(0, 2 * BLK)
    project_out(1, p, own, obuf.at[0], whole)
    for q in range(2):
        part = pl.ds(2 * q * BLK, 2 * BLK)
        for k, lane in enumerate(columns(c)):
            to_partner(OMID + 2 * q + k, obuf.at[0, part, pl.ds(k * BLK, BLK)], o_ref.at[part, lane])
    project_out(1, c, own, obuf.at[1], whole)
    for k, lane in enumerate(columns(c)):
        o_ref[:, lane] = obuf[1, :, k * BLK : (k + 1) * BLK]
    for copies in (near_copies, far_copies):
        for there, copy in zip((has_left, has_right), copies):
            pl.when(there)(copy.wait_send)
    for when, copy in sent:
        if when is None:
            copy.wait_send()
        else:
            pl.when(when)(copy.wait_send)
    pl.when(head)(back_again.wait_send)
    for q in range(2):
        part = pl.ds(2 * q * BLK, 2 * BLK)
        for k, lane in enumerate(columns(p)):
            from_partner(OMID + 2 * q + k, o_ref.at[part, lane])


def scoped(n_sp, *refs):
    pl.run_scoped(
        lambda *semaphores: kernel(n_sp, *refs, *semaphores),
        pltpu.SemaphoreType.DMA((11,)),
        pltpu.SemaphoreType.DMA((22,)),
    )


def write_kernel(src, dst, sem):
    copy = pltpu.make_async_copy(src, dst, sem)
    copy.start()
    copy.wait()


def write_out(value):
    return pl.pallas_call(
        write_kernel,
        out_shape=jax.ShapeDtypeStruct(value.shape, value.dtype),
        in_specs=[pl.BlockSpec(memory_space=pltpu.VMEM)],
        out_specs=pl.BlockSpec(memory_space=pl.ANY),
        scratch_shapes=[pltpu.SemaphoreType.DMA],
        compiler_params=pltpu.CompilerParams(vmem_limit_bytes=1024 * 1024),
    )(pltpu.with_memory_space_constraint(value, pltpu.VMEM))


def solution(mesh):
    n_sp = mesh.shape["sp"]

    def body(stream, norm_gain, w_value, w_gate, conv_taps, group_gain, group_shift, w_out):
        layers, features = norm_gain.shape
        half_features, tokens = stream.shape
        channels = w_value.shape[1]
        taps = conv_taps.shape[2]
        any_spec = pl.BlockSpec(memory_space=pl.ANY)
        vmem = pltpu.VMEM
        result = pl.pallas_call(
            functools.partial(scoped, n_sp),
            out_shape=pltpu.VMEM(stream.shape, stream.dtype),
            in_specs=[any_spec] * 11,
            out_specs=pl.BlockSpec(memory_space=pltpu.VMEM),
            scratch_shapes=[
                vmem((2, half_features, tokens), BF16),
                vmem((2, half_features, 3 * BLK), BF16),
                vmem((layers, 2, 2, BLK, features), BF16),
                vmem((layers, 2, 2, 2, BLK, features), BF16),
                vmem((layers, 2, half_features, 2 * channels), BF16),
                vmem((2 * BLK, layers, channels), BF16),
                vmem((layers, features), F32),
                vmem((2, 2, layers, channels), F32),
                vmem((layers, 2, channels, BLK), F32),
                vmem((layers, 2, channels, BLK), F32),
                vmem((layers, 2, channels, SIZE), BF16),
                vmem((SIZE, SIZE), BF16),
                vmem((SIZE, 2 * BLK), BF16),
                vmem((layers, SIZE, SIZE), BF16),
                vmem((2, 2 * BLK, tokens), F32),
                vmem((2, channels, SIZE), F32),
                vmem((2, channels, SIZE), F32),
                vmem((4, channels, BLK), BF16),
                vmem((2, channels, 3 * BLK), BF16),
                vmem((2, channels, 3 * BLK), BF16),
                vmem((2, channels, BLK), BF16),
                vmem((2, channels, BLK), BF16),
                vmem((2, channels, BLK), BF16),
                vmem((2, channels, BLK), BF16),
                vmem((2, channels, 3 * BLK), BF16),
                vmem((2, half_features, 2 * BLK), BF16),
                pltpu.SemaphoreType.DMA((22,)),
                pltpu.SemaphoreType.REGULAR,
            ],
            compiler_params=pltpu.CompilerParams(
                collective_id=0, has_side_effects=True, vmem_limit_bytes=60 * 1024 * 1024
            ),
        )(
            stream, norm_gain, w_value, w_gate, jnp.transpose(conv_taps, (2, 0, 1)),
            group_gain, group_shift, w_out, *tables(taps),
        )
        return write_out(result)

    placed = (
        P("tp", "sp"),
        P(),
        P(None, "tp", None),
        P(None, "tp", None),
        P(None, "tp", None),
        P(None, "tp"),
        P(None, "tp"),
        P(None, "tp", None),
    )
    return jax.shard_map(body, mesh=mesh, in_specs=placed, out_specs=P("tp", "sp"), check_vma=False)
```

```python
import functools

import jax
import jax.numpy as jnp
import numpy as np
from jax import lax
from jax.experimental import pallas as pl
from jax.experimental.pallas import tpu as pltpu
from jax.sharding import PartitionSpec as P

MESH = pl.DeviceIdType.MESH
BLK = 128
SIZE = 512
HALF = SIZE // 2
RMS_EPS = 1e-06
LN_EPS = 1e-05
F32 = jnp.float32
BF16 = jnp.bfloat16


def tables(taps):
    angle = lambda t: np.asarray(t)[:, None] * ((np.arange(HALF) + 0.5) * (2 * np.pi / SIZE))[None]
    trig = lambda t: np.stack([np.cos(angle(t)), np.sin(angle(t))], axis=1).reshape(
        -1, 2, 2, BLK
    ).transpose(0, 2, 1, 3).reshape(-1, SIZE)
    blocks = [np.arange(BLK) + BLK * b for b in range(4)]
    reach = (taps - 1) // 2
    forward = [np.concatenate([trig(blocks[b]) for b in order]) for order in ((0, 1, 2, 3), (3, 2, 1, 0))]
    back = [
        np.concatenate([trig(blocks[b] - reach).T for b in order], axis=1) * (2.0 / SIZE)
        for order in ((1, 2), (2, 1))
    ]
    mixed = np.zeros((2, 2 * BLK, 2, 2 * HALF))
    for layer in range(2):
        mixed[layer, :taps, layer] = trig(np.arange(taps))
    return (
        jnp.asarray(np.stack(forward), BF16),
        jnp.asarray(np.stack(back), BF16),
        jnp.asarray(mixed.reshape(2, 4 * BLK, SIZE), BF16),
    )


def kernel(
    n_sp,
    x_hbm, ng_hbm, wv_hbm, wg_hbm, taps_hbm, gg_hbm, gs_hbm, wo_hbm, fwd_hbm, back_hbm, ftap_hbm,
    o_ref,
    xall, xs, wraw, wvg, wo, taps, ngv, gv, ggb, gsb, resp, fwd, back, ftap,
    acc, begun, begun_last, gall, g1, g2, gfar, gnear, gpar1, gpar2, act, obuf,
    rsem, ready, lsem, ssem,
):
    sp, c = lax.axis_index("sp"), lax.axis_index("tp")
    p = 1 - c
    outer = sp + 2 * c - 1
    has_left = sp > 0
    has_right = sp < n_sp - 1
    has_outer = jnp.logical_and(outer >= 0, outer < n_sp)
    first = sp == 0
    head = jnp.logical_and(first, c == 0)
    early = jnp.logical_and(first, c == 1)
    later = jnp.logical_not(early)
    past = sp > 0
    slow = jnp.logical_and(past, lax.rem(sp, 16) == 0)
    prompt = jnp.logical_not(slow)
    left_count = jnp.where(has_left, 1, 0)
    right_count = jnp.where(has_right, 1, 0)
    layers, features = ng_hbm.shape

    local = {}

    def load(name, pairs, whole):
        sem = lsem.at[len(local)]
        for src, dst in pairs:
            pltpu.make_async_copy(src, dst, sem).start()
        local[name] = pltpu.make_async_copy(whole, whole, sem)

    def loaded(*names):
        for name in names:
            local[name].wait()

    def load_wvg(l):
        pairs = []
        for k in range(2):
            pairs.append((wv_hbm.at[l, pl.ds(k * BLK, BLK)], wraw.at[l, k, 0]))
            pairs.append((wg_hbm.at[l, pl.ds(k * BLK, BLK)], wraw.at[l, k, 1]))
        load(f"w{l}", pairs, wraw.at[l])

    load("x", [(x_hbm, xall.at[c])], xall.at[c])

    barrier = pltpu.get_barrier_semaphore()
    pl.semaphore_signal(barrier, inc=1, device_id=(sp, p), device_id_type=MESH)

    @pl.when(has_outer)
    def _():
        pl.semaphore_signal(barrier, inc=1, device_id=(outer, 1), device_id_type=MESH)

    load("ng", [(ng_hbm, ngv)], ngv)
    load("groups", [(gg_hbm, gv.at[c, 0]), (gs_hbm, gv.at[c, 1])], gv.at[c])
    load_wvg(0)
    load("wo0", [(wo_hbm.at[0], wo.at[0, c])], wo.at[0, c])
    tap_rows = taps.at[pl.ds(0, taps_hbm.shape[0])]
    load("taps", [(taps_hbm, tap_rows)], tap_rows)
    load("ftap", [(ftap_hbm, ftap)], ftap)
    load_wvg(1)
    load("fwd", [(fwd_hbm.at[c], fwd)], fwd)
    load("back", [(back_hbm.at[c], back)], back)
    load("wo1", [(wo_hbm.at[1], wo.at[1, c])], wo.at[1, c])

    NEAR, FAR, X, GMID, GINN, WVG, WO, RESP, GV, PAR1, PAR2, OMID = 0, 2, 4, 5, 6, 7, 9, 11, 13, 14, 15, 16
    FORTH, BACK = 20, 21
    sent = []

    def remote(k, src, dst, device):
        return pltpu.make_async_remote_copy(
            src_ref=src, dst_ref=dst, send_sem=ssem.at[k], recv_sem=rsem.at[k],
            device_id=device, device_id_type=MESH,
        )

    def to_partner(k, src, dst, when=None):
        copy = remote(k, src, dst, (sp, p))
        if when is None:
            copy.start()
        else:
            pl.when(when)(copy.start)
        if when is not later:
            sent.append((None if when is early else when, copy))

    def share(ref, k, l, when=None):
        to_partner(k + l, ref.at[l, c], ref.at[l, c], when)

    def from_partner(k, dst):
        remote(k, dst, dst, (sp, p)).wait_recv()

    def to_neighbour(first, direction, src, dst):
        return pltpu.make_async_remote_copy(
            src_ref=src, dst_ref=dst, send_sem=ssem.at[first + direction], recv_sem=rsem.at[first + c],
            device_id=(sp + 2 * direction - 1, 1 - direction), device_id_type=MESH,
        )

    def from_outer(first, part):
        for core in range(2):
            dst = part(core)
            pltpu.make_async_remote_copy(
                src_ref=dst, dst_ref=dst, send_sem=ssem.at[first], recv_sem=rsem.at[first + core],
                device_id=(outer, core), device_id_type=MESH,
            ).wait_recv()

    def start_both(copies):
        for there, copy in zip((has_left, has_right), copies):
            pl.when(there)(copy.start)

    def scale_weights(l):
        gain = ngv[l : l + 1]
        for k in range(2):
            for half in range(2):
                wvg[l, c, k, half] = (wraw[l, k, half].astype(F32) * gain).astype(BF16)

    def spread_groups(h):
        column = lambda row: jnp.broadcast_to(row * 0.5, (BLK, BLK)).T
        for l in range(layers):
            for b in range(2):
                lanes = slice(b * BLK, (b + 1) * BLK)
                ggb[l, h, lanes] = column(gv[h, 0, l : l + 1, lanes])
                gsb[l, h, lanes] = column(gv[h, 1, l : l + 1, lanes])

    def prepare_gates():
        loaded("groups")
        spread_groups(c)
        loaded("ng", "w0")
        scale_weights(0)

    def prepare_taps():
        loaded("taps", "ftap")
        taps[taps_hbm.shape[0] :] = jnp.zeros((taps.shape[0] - taps_hbm.shape[0], *taps.shape[1:]), BF16)

    def respond(l):
        rows = taps[...].reshape(layers * taps.shape[0], taps.shape[2])
        resp[l, c] = lax.dot_general(
            rows, ftap[l], (((0,), (0,)), ((), ())), preferred_element_type=F32
        ).astype(BF16)

    def prepare_weights():
        loaded("w1")
        scale_weights(1)

    @pl.when(early)
    def _():
        prepare_gates()
        prepare_taps()
        for l in range(layers):
            respond(l)
        prepare_weights()

    @pl.when(c == 0)
    def _():
        pl.semaphore_wait(barrier, 1)
        pl.semaphore_signal(ready, inc=1, device_id=(sp, 1), device_id_type=MESH)

    @pl.when(c == 1)
    def _():
        pl.semaphore_wait(ready, 1)

    loaded("x")
    to_partner(X, xall.at[c], xall.at[c])
    wo_copy = remote(WO, wo.at[0, c], wo.at[0, c], (sp, p))
    wvg_copy = remote(WVG, wvg.at[0, c], wvg.at[0, c], (sp, p))
    sent.extend([(None, wo_copy), (past, wvg_copy)])

    @pl.when(slow)
    def _():
        loaded("wo0")
        wo_copy.start()
        prepare_gates()
        wvg_copy.start()

    @pl.when(c == 1)
    def _():
        pl.semaphore_wait(barrier, 1 + left_count + right_count)
        pl.semaphore_signal(ready, inc=1, device_id=(sp, 0), device_id_type=MESH)

    @pl.when(c == 0)
    def _():
        pl.semaphore_wait(ready, 1)

    near = (slice(None), pl.ds(0, BLK))
    near_copies = [to_neighbour(NEAR, d, xall.at[c, :, pl.ds(3 * d * BLK, BLK)], xs.at[(c, *near)]) for d in range(2)]
    start_both(near_copies)

    pl.when(jnp.logical_and(later, prompt))(prepare_gates)
    to_partner(GV, gv.at[c], gv.at[c])

    @pl.when(prompt)
    def _():
        loaded("wo0")
        wo_copy.start()

    for l in range(layers):
        share(resp, RESP, l, early)

    def squares(x):
        wide = x.astype(F32)
        return jnp.sum(wide * wide, axis=0, keepdims=True)

    def half_inverse(total):
        return 0.5 * lax.rsqrt(total * (1.0 / features) + RMS_EPS)

    def gated(r, inverse):
        value = r[:BLK] * inverse
        return (value * jnp.tanh(r[BLK:] * inverse) + value).astype(BF16)

    def gate(l, lanes, dst, arrived=None, halves=(0, 1)):
        x = xs[:, :, lanes].reshape(features, lanes.stop - lanes.start)
        inverse = half_inverse(squares(x))
        for h in halves if arrived is None else (c, p):
            if h is p:
                arrived()
            for k in range(2):
                r = jnp.dot(wvg[l, h, k].reshape(2 * BLK, features), x, preferred_element_type=F32)
                dst[h, k * BLK : (k + 1) * BLK, lanes] = gated(r, inverse)

    def begin_filter(begun, ready):
        for h in range(2):
            for q in range(2):
                both = slice(2 * q * BLK, 2 * (q + 1) * BLK)
                begun[h, :, both] = jnp.dot(ready(h), fwd[2 * BLK :, both], preferred_element_type=F32)

    def filter_norm(l, window, outputs, lanes, halves=(0, 1), begun=None):
        n = outputs.stop - outputs.start
        for h in halves:
            w = window(h)
            filtered = None
            for q in range(2):
                both, re, im = (slice(2 * q * BLK + i * BLK, 2 * q * BLK + j * BLK) for i, j in ((0, 2), (0, 1), (1, 2)))
                g = jnp.dot(w, fwd[: w.shape[1], both], preferred_element_type=F32)
                if begun is not None:
                    g = g + begun[h, :, both]
                gr, gi = g[:, :BLK], g[:, BLK:]
                hr, hi = resp[l, h, :, re].astype(F32), resp[l, h, :, im].astype(F32)
                y = jnp.concatenate([(gr * hr + gi * hi).astype(BF16), (gi * hr - gr * hi).astype(BF16)], axis=1)
                term = jnp.dot(y, back[both, outputs], preferred_element_type=F32)
                filtered = term if filtered is None else filtered + term
            for k in range(2):
                part = slice(k * BLK, (k + 1) * BLK)
                f = filtered[part]
                centred = f - jnp.sum(f, axis=0, keepdims=True) * (1.0 / BLK)
                variance = jnp.sum(centred * centred, axis=0, keepdims=True) * (1.0 / BLK)
                gain, shift = ggb[l, h, part], gsb[l, h, part]
                if n > BLK:
                    gain = jnp.concatenate([gain] * (n // BLK), axis=1)
                    shift = jnp.concatenate([shift] * (n // BLK), axis=1)
                s = centred * lax.rsqrt(variance + LN_EPS) * gain + shift
                act[h, part, lanes] = (s * jnp.tanh(s) + s).astype(BF16)

    def project_out(l, h, lanes, dst, dst_lanes, pieces=((0, 2 * BLK), (2 * BLK, 2 * BLK))):
        for first, size in pieces:
            part = slice(first, first + size)
            branch = None
            for g in range(2):
                group = slice(g * 2 * BLK, (g + 1) * 2 * BLK)
                term = jnp.dot(wo[l, h, part, group], act[g, :, lanes], preferred_element_type=F32)
                branch = term if branch is None else branch + term
            dst[part, dst_lanes] = (xs[h, part, lanes].astype(F32) + branch).astype(BF16)

    def advance(l, lanes):
        for h in range(2):
            project_out(l, h, lanes, xs.at[h], lanes)

    columns = lambda core: (
        pl.ds(pl.multiple_of(core * 3 * BLK, BLK), BLK),
        pl.ds(pl.multiple_of((1 + core) * BLK, BLK), BLK),
    )
    own, outside = slice(BLK, 3 * BLK), slice(0, BLK)
    inner, outward = slice(2 * BLK, 3 * BLK), slice(0, 2 * BLK)

    part_rows = features // 2

    def part_dot(core, k):
        x = xall[core]
        w = wvg[0, c, k, :, :, pl.ds(pl.multiple_of(core * part_rows, part_rows), part_rows)]
        return jnp.dot(w.reshape(2 * BLK, part_rows), x, preferred_element_type=F32)

    def part_squares(core):
        return squares(xall[core])

    for k in range(2):
        acc[k] = part_dot(c, k)
    total = part_squares(c)
    near_block = xs.at[(slice(None), *near)]
    forth = remote(FORTH, near_block, near_block, (sp, p))
    back_again = remote(BACK, gnear.at[c], g1.at[(c, *near)], (sp, p))

    @pl.when(early)
    def _():
        from_outer(NEAR, lambda core: xs.at[(core, *near)])
        forth.start()
        gate(0, outside, g1, halves=(c,))

    from_partner(X, xall.at[p])
    inverse = half_inverse(total + part_squares(p))
    for k in range(2):
        gk = gated(acc[k] + part_dot(p, k), inverse)
        for b in range(4):
            gall[b, k * BLK : (k + 1) * BLK] = gk[:, b * BLK : (b + 1) * BLK]
    mid, inn = pl.ds(BLK, BLK), pl.ds(2 * BLK, BLK)
    to_partner(GINN, gall.at[1 + p], g1.at[c, :, inn])
    to_partner(PAR1, gall.at[1 + c], gpar1.at[c])
    to_partner(GMID, gall.at[3 * p], g1.at[c, :, mid])
    far_copies = [to_neighbour(FAR, d, gall.at[1 + d], gfar.at[c]) for d in range(2)]
    start_both(far_copies)

    @pl.when(later)
    def _():
        prepare_taps()
        respond(0)

    share(resp, RESP, 0, later)
    pl.when(later)(prepare_weights)
    share(wvg, WVG, 1)
    pl.when(jnp.logical_and(past, prompt))(wvg_copy.start)
    for h in range(2):
        for place, lane in zip((1, 2), columns(c)):
            xs[h, :, place * BLK : (place + 1) * BLK] = xall[h, :, lane]
    g1[c, :, BLK : 2 * BLK] = gall[3 * c]
    g1[c, :, 2 * BLK : 3 * BLK] = gall[1 + c]
    gpar1[c] = gall[1 + p]

    loaded("fwd", "back")

    inner_window = lambda h: jnp.concatenate([g1[h, :, own], gpar1[h]], axis=1)
    alone = jnp.logical_not(has_outer)
    inside = jnp.logical_and(has_outer, past)

    @pl.when(has_outer)
    def _():
        filter_norm(0, inner_window, slice(0, BLK), inner, (c,))

    from_partner(GV, gv.at[p])
    spread_groups(p)

    @pl.when(head)
    def _():
        forth.wait_recv()
        gate(0, outside, gnear, halves=(c,))
        back_again.start()

    from_partner(RESP, resp.at[0, p])
    from_partner(WO, wo.at[0, p])
    from_partner(GINN, g1.at[p, :, inn])
    from_partner(PAR1, gpar1.at[p])
    from_partner(GMID, g1.at[p, :, mid])

    @pl.when(has_outer)
    def _():
        def layer_1_weights():
            begin_filter(begun, lambda h: g1[h, :, own])
            from_partner(WVG + 1, wvg.at[1, p])

        filter_norm(0, inner_window, slice(0, BLK), inner, (p,))
        advance(0, inner)
        gate(1, inner, g2, arrived=layer_1_weights)

    @pl.when(alone)
    def _():
        pl.when(past)(lambda: from_partner(WVG, wvg.at[0, p]))
        g1[:, :, outside] = jnp.zeros_like(gfar)
        filter_norm(0, lambda h: jnp.concatenate([g1[h], gpar1[h]], axis=1), slice(0, 2 * BLK), own)
        advance(0, own)
        from_partner(WVG + 1, wvg.at[1, p])
        gate(1, own, g2)
        g2[:, :, outside] = jnp.zeros_like(gfar)

    to_partner(PAR2, g2.at[:, :, inn], gpar2)
    pl.when(later)(lambda: respond(1))
    share(resp, RESP, 1, later)
    loaded("wo1")
    share(wo, WO, 1)

    def begin_last():
        from_partner(PAR2, gpar2)
        begin_filter(begun_last, lambda h: jnp.concatenate([g2[h, :, inner], gpar2[h]], axis=1))

    @pl.when(early)
    def _():
        from_partner(BACK, g1.at[(p, *near)])
        forth.wait_send()

    @pl.when(inside)
    def _():
        from_partner(WVG, wvg.at[0, p])
        from_outer(NEAR, lambda core: xs.at[(core, *near)])
        gate(0, outside, g1)
        begin_last()

    @pl.when(has_outer)
    def _():
        from_outer(FAR, lambda core: gfar.at[core])
        late = lambda h: jnp.concatenate([gfar[h], g1[h, :, outside]], axis=1)
        filter_norm(0, late, slice(0, 2 * BLK), outward, begun=begun)
        advance(0, outward)
        gate(1, outward, g2)

    pl.when(jnp.logical_not(inside))(begin_last)
    from_partner(RESP + 1, resp.at[1, p])
    filter_norm(1, lambda h: g2[h, :, outward], slice(0, 2 * BLK), own, begun=begun_last)
    from_partner(WO + 1, wo.at[1, p])

    whole = slice(0, 2 * BLK)
    project_out(1, p, own, obuf.at[0], whole)
    for q in range(2):
        part = pl.ds(2 * q * BLK, 2 * BLK)
        for k, lane in enumerate(columns(c)):
            to_partner(OMID + 2 * q + k, obuf.at[0, part, pl.ds(k * BLK, BLK)], o_ref.at[part, lane])
    project_out(1, c, own, obuf.at[1], whole)
    for k, lane in enumerate(columns(c)):
        o_ref[:, lane] = obuf[1, :, k * BLK : (k + 1) * BLK]
    for copies in (near_copies, far_copies):
        for there, copy in zip((has_left, has_right), copies):
            pl.when(there)(copy.wait_send)
    for when, copy in sent:
        if when is None:
            copy.wait_send()
        else:
            pl.when(when)(copy.wait_send)
    pl.when(head)(back_again.wait_send)
    for q in range(2):
        part = pl.ds(2 * q * BLK, 2 * BLK)
        for k, lane in enumerate(columns(p)):
            from_partner(OMID + 2 * q + k, o_ref.at[part, lane])


def scoped(n_sp, *refs):
    pl.run_scoped(
        lambda *semaphores: kernel(n_sp, *refs, *semaphores),
        pltpu.SemaphoreType.DMA((11,)),
        pltpu.SemaphoreType.DMA((22,)),
    )


def write_kernel(src, dst, sem):
    copy = pltpu.make_async_copy(src, dst, sem)
    copy.start()
    copy.wait()


def write_out(value):
    return pl.pallas_call(
        write_kernel,
        out_shape=jax.ShapeDtypeStruct(value.shape, value.dtype),
        in_specs=[pl.BlockSpec(memory_space=pltpu.VMEM)],
        out_specs=pl.BlockSpec(memory_space=pl.ANY),
        scratch_shapes=[pltpu.SemaphoreType.DMA],
        compiler_params=pltpu.CompilerParams(vmem_limit_bytes=1024 * 1024),
    )(pltpu.with_memory_space_constraint(value, pltpu.VMEM))


def solution(mesh):
    n_sp = mesh.shape["sp"]

    def body(stream, norm_gain, w_value, w_gate, conv_taps, group_gain, group_shift, w_out):
        layers, features = norm_gain.shape
        half_features, tokens = stream.shape
        channels = w_value.shape[1]
        taps = conv_taps.shape[2]
        any_spec = pl.BlockSpec(memory_space=pl.ANY)
        vmem = pltpu.VMEM
        result = pl.pallas_call(
            functools.partial(scoped, n_sp),
            out_shape=pltpu.VMEM(stream.shape, stream.dtype),
            in_specs=[any_spec] * 11,
            out_specs=pl.BlockSpec(memory_space=pltpu.VMEM),
            scratch_shapes=[
                vmem((2, half_features, tokens), BF16),
                vmem((2, half_features, 3 * BLK), BF16),
                vmem((layers, 2, 2, BLK, features), BF16),
                vmem((layers, 2, 2, 2, BLK, features), BF16),
                vmem((layers, 2, half_features, 2 * channels), BF16),
                vmem((2 * BLK, layers, channels), BF16),
                vmem((layers, features), F32),
                vmem((2, 2, layers, channels), F32),
                vmem((layers, 2, channels, BLK), F32),
                vmem((layers, 2, channels, BLK), F32),
                vmem((layers, 2, channels, SIZE), BF16),
                vmem((SIZE, SIZE), BF16),
                vmem((SIZE, 2 * BLK), BF16),
                vmem((layers, SIZE, SIZE), BF16),
                vmem((2, 2 * BLK, tokens), F32),
                vmem((2, channels, SIZE), F32),
                vmem((2, channels, SIZE), F32),
                vmem((4, channels, BLK), BF16),
                vmem((2, channels, 3 * BLK), BF16),
                vmem((2, channels, 3 * BLK), BF16),
                vmem((2, channels, BLK), BF16),
                vmem((2, channels, BLK), BF16),
                vmem((2, channels, BLK), BF16),
                vmem((2, channels, BLK), BF16),
                vmem((2, channels, 3 * BLK), BF16),
                vmem((2, half_features, 2 * BLK), BF16),
                pltpu.SemaphoreType.DMA((22,)),
                pltpu.SemaphoreType.REGULAR,
            ],
            compiler_params=pltpu.CompilerParams(
                collective_id=0, has_side_effects=True, vmem_limit_bytes=60 * 1024 * 1024
            ),
        )(
            stream, norm_gain, w_value, w_gate, jnp.transpose(conv_taps, (2, 0, 1)),
            group_gain, group_shift, w_out, *tables(taps),
        )
        return write_out(result)

    placed = (
        P("tp", "sp"),
        P(),
        P(None, "tp", None),
        P(None, "tp", None),
        P(None, "tp", None),
        P(None, "tp"),
        P(None, "tp"),
        P(None, "tp", None),
    )
    return jax.shard_map(body, mesh=mesh, in_specs=placed, out_specs=P("tp", "sp"), check_vma=False)
```
